256 devices in a mesh: grp: 2 (over y), fs: 16 (over z), tp: 8 (over x, core).
Axes of the slice: x: 4, y: 2, z: 16, core: 2. Of those that a mesh axis runs over, the one named last changes fastest.
The devices are a block of a 4x16x16 slice.
Arguments:
- tokens: bfloat16 [32768, 2048], P(('grp', 'fs'), 'tp'), parts along dimension 0, may hold values from -6 to 6
- norm1_gain: float32 [2048], replicated, may hold values from 0.1 to 1.9
- weight_u: float32 [2048, 1024], P('fs', 'tp'), may hold values from -0.125 to 0.125
- weight_v: float32 [2048, 1024], P('fs', 'tp'), may hold values from -0.125 to 0.125
- scale_u: float32 [1024], P('tp'), may hold values from 0.5 to 2
- scale_v: float32 [1024], P('tp'), may hold values from 0.05 to 4.5
- mix_gain: float32 [1024], P('tp'), may hold values from 0.1 to 1.9
- spatial_weight: float32 [4, 128, 128], replicated, may hold values from -0.5 to 0.5
- spatial_bias: float32 [4, 128], replicated, may hold values from 0.5 to 1.5
- weight_out: float32 [1024, 2048], P('tp', 'fs'), may hold values from -0.1875 to 0.1875
- scale_out: float32 [2048], P('fs'), may hold values from 0.5 to 2
- norm2_gain: float32 [2048], replicated, may hold values from 0.1 to 1.9
- weight_up: float32 [2048, 8192], P('fs', 'tp'), may hold values from -0.125 to 0.125
- scale_up: float32 [8192], P('tp'), may hold values from 0.5 to 2
- weight_down: float32 [8192, 2048], P('tp', 'fs'), may hold values from -0.0625 to 0.0625
- scale_down: float32 [2048], P('fs'), may hold values from 0.5 to 2
Outputs:
- result: bfloat16 [32768, 2048], P(('grp', 'fs'), 'tp'), parts along dimension 0
The draws below stay inside these ranges and needn't reach their ends.
There are 2 independent parts, one for each index of `grp`. The reference program is written for one: setup_inputs(seed, part) draws one part's arguments, and reference() takes and returns one part's arrays. A program takes and returns all parts, laid end to end along the dimension named above; an argument that names none is the same for every part. Nothing has to cross between parts.
All inputs are finite; a program needn't handle non-finite values.
Results may differ from the reference program's by a relative error of at most 0.023.
Values may be sent and summed in bfloat16 or wider, within the bound.
A program may use at most 128 MiB of HBM per device.

```python
import math
import jax
import jax.numpy as jnp
from jax import lax

D = 2048
GM_W = 1024
GROUPS = 4
BLOCK = 128
FF = 8192
TOKENS = 16384
N_TP = 8


def draw_scale_v(key, part):
    columns = jnp.arange(GM_W, dtype=jnp.float32) / GM_W
    roughness = jax.random.uniform(key, (GM_W,), jnp.float32, 0.5, 1.5)
    return 0.4 * jnp.exp(columns * jnp.log(4.0)) * roughness


def level_of(stream_key, dims, split, least, top_value):
    gain, own = 1.0, jax.random.fold_in(stream_key, 6)
    for axis_at, blocks in split:
        heights = jnp.exp(jax.random.uniform(jax.random.fold_in(own, axis_at), (blocks,), jnp.float32, least / len(split), top_value / len(split)))
        gain = gain * jnp.repeat(heights, dims[axis_at] // blocks).reshape([-1 if axis == axis_at else 1 for axis in range(len(dims))])
    return gain


def bell_draw(stream_key, dims, spread, limit, cuts=(), kind=jnp.bfloat16):
    entries = spread * jax.random.normal(stream_key, dims, jnp.float32)
    if cuts:
        entries = entries * level_of(stream_key, dims, cuts, -0.22, 0.18)
    return jnp.clip(entries, -limit, limit).astype(kind)


def setup_inputs(seed: int = 0, part: int = 0) -> dict:
    seeds = jax.random.split(jax.random.key(seed), 17)
    part_keys = jax.random.split(jax.random.fold_in(seeds[16], part), 17)
    tokens = bell_draw(part_keys[0], (TOKENS, D), 1.0, 6.0, ((0, 16), (1, 8)))
    norm1_gain = jnp.clip(1.0 + 0.18 * jax.random.normal(seeds[1], (D,), jnp.float32), 0.1, 1.9)
    weight_u = bell_draw(seeds[2], (D, GM_W), D ** -0.5, 0.125, ((0, 16), (1, 8)), jnp.float32)
    weight_v = bell_draw(seeds[3], (D, GM_W), D ** -0.5, 0.125, ((0, 16), (1, 8)), jnp.float32)
    scale_u = jnp.clip(jnp.exp(math.log(2.0) - 1.3862944 * jax.random.uniform(seeds[4], (GM_W,), jnp.float32) ** level_of(seeds[4], (GM_W,), ((0, 8),), -0.2, 0.2)), 0.5, 2.0)
    scale_v = draw_scale_v(jax.random.fold_in(seeds[16], 71), part)
    mix_gain = jnp.clip(1.0 + 0.18 * jax.random.normal(seeds[6], (GM_W,), jnp.float32), 0.1, 1.9)
    spatial_weight = bell_draw(seeds[7], (GROUPS, BLOCK, BLOCK), BLOCK ** -0.5, 0.5, (), jnp.float32)
    spatial_bias = jnp.clip(jax.random.uniform(seeds[8], (GROUPS, BLOCK), jnp.float32, 0.5, 1.5), 0.5, 1.5)
    weight_out = bell_draw(seeds[9], (GM_W, D), GM_W ** -0.5, 0.1875, ((0, 8), (1, 16)), jnp.float32)
    scale_out = jnp.clip(jnp.exp(math.log(2.0) - 1.3862944 * jax.random.uniform(seeds[10], (D,), jnp.float32) ** level_of(seeds[10], (D,), ((0, 16),), -0.2, 0.2)), 0.5, 2.0)
    norm2_gain = jnp.clip(1.0 + 0.18 * jax.random.normal(seeds[11], (D,), jnp.float32), 0.1, 1.9)
    weight_up = bell_draw(seeds[12], (D, FF), D ** -0.5, 0.125, ((0, 16), (1, 8)), jnp.float32)
    scale_up = jnp.clip(jnp.exp(math.log(2.0) - 1.3862944 * jax.random.uniform(seeds[13], (FF,), jnp.float32) ** level_of(seeds[13], (FF,), ((0, 8),), -0.2, 0.2)), 0.5, 2.0)
    weight_down = bell_draw(seeds[14], (FF, D), FF ** -0.5, 0.0625, ((0, 8), (1, 16)), jnp.float32)
    scale_down = jnp.clip(jnp.exp(math.log(2.0) - 1.3862944 * jax.random.uniform(seeds[15], (D,), jnp.float32) ** level_of(seeds[15], (D,), ((0, 16),), -0.2, 0.2)), 0.5, 2.0)
    return {"tokens": tokens, "norm1_gain": norm1_gain, "weight_u": weight_u, "weight_v": weight_v, "scale_u": scale_u, "scale_v": scale_v, "mix_gain": mix_gain, "spatial_weight": spatial_weight, "spatial_bias": spatial_bias, "weight_out": weight_out, "scale_out": scale_out, "norm2_gain": norm2_gain, "weight_up": weight_up, "scale_up": scale_up, "weight_down": weight_down, "scale_down": scale_down}


def rms_rows(values, gain_vector):
    widened = values.astype(jnp.float32)
    scaled = widened * lax.rsqrt(lax.optimization_barrier(jnp.mean(widened * widened, axis=-1, keepdims=True)) + 1e-06)
    return (scaled * gain_vector).astype(jnp.bfloat16)

def run_sum(operand_left, operand_right, column_scale, pieces):
    run_width = operand_left.shape[1] // pieces
    running = jnp.zeros((operand_left.shape[0], operand_right.shape[1]), jnp.float32)
    for run_index in range(pieces):
        lower = run_index * run_width
        partial_term = jnp.dot(operand_left[:, lower:lower + run_width], operand_right[lower:lower + run_width], preferred_element_type=jnp.float32) * column_scale
        running = running + lax.optimization_barrier(partial_term.astype(jnp.bfloat16)).astype(jnp.float32)
    return running

def reference(tokens, norm1_gain, weight_u, weight_v, scale_u, scale_v, mix_gain, spatial_weight, spatial_bias, weight_out, scale_out, norm2_gain, weight_up, scale_up, weight_down, scale_down):
    normed_in = rms_rows(tokens, norm1_gain)
    pre_u = jnp.dot(normed_in, weight_u.astype(jnp.bfloat16), preferred_element_type=jnp.float32) * scale_u
    pre_v = jnp.dot(normed_in, weight_v.astype(jnp.bfloat16), preferred_element_type=jnp.float32) * scale_v
    gate_u = jax.nn.gelu(pre_u)
    act_v = jax.nn.gelu(pre_v)
    row_mean = lax.optimization_barrier(jnp.mean(act_v, axis=-1, keepdims=True))
    square = lax.optimization_barrier(jnp.mean(act_v * act_v, axis=-1, keepdims=True))
    v_norm = ((act_v - row_mean) * lax.rsqrt(square - row_mean * row_mean + 1e-06) * mix_gain).astype(jnp.bfloat16)
    lower_mask = jnp.tril(jnp.ones((BLOCK, BLOCK), jnp.float32))
    spatial_mask = (spatial_weight * lower_mask).astype(jnp.bfloat16)
    blocks = v_norm.reshape(TOKENS // BLOCK, BLOCK, GROUPS, GM_W // GROUPS)
    mixed_cols = jnp.einsum('gts,nsgc->ntgc', spatial_mask.astype(jnp.float32), blocks.astype(jnp.float32))
    mixed_cols = mixed_cols + spatial_bias.T[None, :, :, None]
    gated = (gate_u * mixed_cols.reshape(TOKENS, GM_W)).astype(jnp.bfloat16)
    mixer_sum = run_sum(gated, weight_out.astype(jnp.bfloat16), scale_out, N_TP)
    residual = (tokens.astype(jnp.float32) + mixer_sum).astype(jnp.bfloat16)
    normed_mid = rms_rows(residual, norm2_gain)
    pre_up = jnp.dot(normed_mid, weight_up.astype(jnp.bfloat16), preferred_element_type=jnp.float32) * scale_up
    hidden = jnp.square(jax.nn.relu(pre_up)).astype(jnp.bfloat16)
    channel_sum = run_sum(hidden, weight_down.astype(jnp.bfloat16), scale_down, N_TP)
    return (residual.astype(jnp.float32) + channel_sum).astype(jnp.bfloat16)
```

```python
import functools

import jax
import jax.numpy as jnp
from jax import lax
from jax.experimental import pallas as pl
from jax.experimental.pallas import tpu as pltpu
from jax.sharding import PartitionSpec as P

BF = jnp.bfloat16
F32 = jnp.float32
MESH = pl.DeviceIdType.MESH
EPS = 1e-06
CORES = 2
CHUNKS = 2
ROWS = 256


class Stream:
    def __init__(self, name, ref, rows, whole, paired):
        self.name, self.ref, self.rows, self.whole, self.paired = name, ref, rows, whole, paired


def kernel(
    dims,
    x_ref, g1_ref, wu_ref, wv_ref, suv_ref, mg_ref, sw_ref, sb_ref, wo_ref, so_ref,
    g2_ref, wup_ref, sup_ref, wdn_ref, sdn_ref,
    out_ref,
    wuv, wout, wup, wdn, xg, rg, ub, vt, st_own, st_p, st_c, st_x, gated, hid,
    ps1, pr1, qs1, op1, fi1, ps2, pr2, qs2, op2, fi2, mask, bias,
    z_recv, z_send, y_recv, y_send, ag_recv, ag_send, agp_recv, agp_send,
    rp_recv, rp_send, rr_recv, rr_send, st_recv, st_send,
):
    n_fs, n_tp = dims["fs"], dims["tp"]
    n_x = n_tp // CORES
    half_ring = n_fs // 2
    total_rows, width = x_ref.shape
    feats = width * n_tp
    u_w = wu_ref.shape[1]
    k_fs = wu_ref.shape[0]
    h_w = wup_ref.shape[1]
    gm_w = u_w * n_tp
    chunk = total_rows // CHUNKS
    half = chunk // 2
    block = sw_ref.shape[1]
    pair = dims["grp"] % 2 == 0

    g = lax.axis_index("grp")
    f = lax.axis_index("fs")
    t = lax.axis_index("tp")
    cx = t // CORES
    core = t % CORES
    par = g % 2

    def chip(d):
        return (cx + d) % n_x

    def tp_of(d):
        return chip(d) * CORES + core

    to_right, to_left, to_opp = {"tp": tp_of(1)}, {"tp": tp_of(n_x - 1)}, {"tp": tp_of(2)}
    to_mate = {"tp": cx * CORES + 1 - core}
    to_up, to_down = {"fs": (f + 1) % n_fs}, {"fs": (f + n_fs - 1) % n_fs}
    to_pair = {"grp": g + 1 - 2 * par}

    neighbours = [to_right, to_left, to_opp, to_mate, to_up, to_down]
    if pair:
        neighbours.append(to_pair)
    barrier = pltpu.get_barrier_semaphore()
    for n in neighbours:
        pl.semaphore_signal(barrier, inc=1, device_id=n, device_id_type=MESH)
    pl.semaphore_wait(barrier, len(neighbours))

    def rcopy(src, dst, ss, rs, dev):
        return pltpu.make_async_remote_copy(
            src_ref=src, dst_ref=dst, send_sem=ss, recv_sem=rs, device_id=dev, device_id_type=MESH)

    def got(ref, sem, spare, dev):
        rcopy(ref, ref, spare, sem, dev).wait_recv()

    def sent(ref, sem, spare, dev):
        rcopy(ref, ref, sem, spare, dev).wait_send()

    def rows_2d(ref, start):
        def at(slot, rows):
            return ref.at[pl.ds(pl.multiple_of(slot * k_fs + start, 16), rows), :]
        return at

    def rows_3d(ref, start):
        def at(slot, rows):
            return ref.at[slot, pl.ds(pl.multiple_of(start, 16), rows), :]
        return at

    def whole_2d(ref, rows):
        return ref.at[pl.ds(0, (n_fs - 1) * rows), :]

    def whole_3d(ref, rows):
        return ref.at[pl.ds(0, n_fs - 1), pl.ds(0, rows), :]

    def make(name, ref, three, own_rows, swap):
        at, whole = (rows_3d, whole_3d) if three else (rows_2d, whole_2d)
        result = []
        if pair and swap:
            shared = own_rows - 2 * swap
            result.append(Stream(name + "y", at(ref, par * (own_rows - swap)), swap, whole(ref, swap), True))
            result.append(Stream(name + "b", at(ref, swap), shared, whole(ref, shared), False))
        else:
            result.append(Stream(name, at(ref, 0), own_rows, whole(ref, own_rows), False))
        return result

    streams = {}
    for s in (make("uv", wuv, False, k_fs, 0) + make("out", wout, True, wo_ref.shape[0], 0)
              + make("up", wup, False, k_fs, 48) + make("dn", wdn, True, h_w, 416)):
        s.index = len(streams)
        streams[s.name] = s

    def z_dirs(s, hop):
        return (0, 1) if hop < half_ring else (s.index % 2,)

    def z_hop(name, hop):
        s = streams[name]
        for d in (0, 1):
            to = to_up if d == 0 else to_down
            if hop > 1 and d in z_dirs(s, hop - 1):
                back = hop - 1
                slot = (f + (n_fs - back if d == 0 else back)) % n_fs
                piece = s.ref(slot, s.rows)
                got(piece, z_recv.at[s.index, d, hop - 2], z_send.at[s.index], to)
                if s.paired:
                    rcopy(piece, piece, y_send.at[s.index], y_recv.at[s.index], to_pair).start()
            if hop <= half_ring and d in z_dirs(s, hop):
                back = hop - 1
                slot = (f + (n_fs - back if d == 0 else back)) % n_fs
                piece = s.ref(slot, s.rows)
                rcopy(piece, piece, z_send.at[s.index], z_recv.at[s.index, d, hop - 1], to).start()

    def y_done(name):
        s = streams[name]
        got(s.whole, y_recv.at[s.index], y_send.at[s.index], to_pair)

    def ag_rows(buf, slot, start, rows):
        return buf.at[slot, pl.ds(start, rows), :]

    def ag_a(ph, k, src, buf):
        rows = src(k * chunk, chunk)
        dst = ag_rows(buf, t, k * chunk, chunk)
        rcopy(rows, dst, ag_send.at[ph, k], ag_recv.at[ph, k, 0], to_right).start()
        rcopy(rows, dst, ag_send.at[ph, k], ag_recv.at[ph, k, 1], to_left).start()
        rcopy(rows, dst, agp_send.at[ph, k], agp_recv.at[ph, k], to_mate).start()

    def to_other_core(ph, k, piece):
        rcopy(piece, piece, agp_send.at[ph, k], agp_recv.at[ph, k], to_mate).start()

    def ag_b(ph, k, buf):
        for d, src_chip, lo, to in ((0, n_x - 1, 0, to_right), (1, 1, half, to_left)):
            slot = tp_of(src_chip)
            piece = ag_rows(buf, slot, k * chunk, chunk)
            got(piece, ag_recv.at[ph, k, d], ag_send.at[ph, k], to)
            part = ag_rows(buf, slot, k * chunk + lo, half)
            rcopy(part, part, ag_send.at[ph, k], ag_recv.at[ph, k, 2 + d], to).start()
            to_other_core(ph, k, piece)

    def ag_c(ph, k, buf):
        slot = tp_of(2)
        for d, lo in ((0, 0), (1, half)):
            part = ag_rows(buf, slot, k * chunk + lo, half)
            got(part, ag_recv.at[ph, k, 2 + d], ag_send.at[ph, k], to_right)
            to_other_core(ph, k, part)

    def ag_d(ph, k, buf):
        got(buf.at[pl.ds(0, n_x), pl.ds(k * chunk, chunk), :], agp_recv.at[ph, k], agp_send.at[ph, k], to_mate)

    def dest(w, rel, c):
        j = chip(rel) * CORES + c
        return jnp.concatenate([w[2 * j], w[2 * j + 1]], axis=1)

    ORDER = (2, 1, 3, 0)
    bufs = ((ps1, pr1, qs1, op1, fi1), (ps2, pr2, qs2, op2, fi2))

    def rs_a(ph, k, lhs, w):
        ps, pr = bufs[ph][:2]
        for rel in ORDER:
            right = dest(w, rel, 1 - core)

            def body(i, _):
                r = pl.multiple_of(i * ROWS, ROWS)
                ps[k, rel, pl.ds(r, ROWS), :] = jnp.dot(
                    lhs[pl.ds(k * chunk + r, ROWS), :], right, preferred_element_type=F32).astype(BF)
                return 0

            lax.fori_loop(0, chunk // ROWS, body, 0)
            rcopy(ps.at[k, rel], pr.at[k, rel], rp_send.at[ph, k], rp_recv.at[ph, k, rel], to_mate).start()

    def rs_b(ph, k, lhs, w):
        ps, pr, qs, op, fi = bufs[ph]
        for rel in ORDER:
            right = dest(w, rel, core)
            got(pr.at[k, rel], rp_recv.at[ph, k, rel], rp_send.at[ph, k], to_mate)

            def body(i, _):
                r = pl.multiple_of(i * ROWS, ROWS)
                qs[k, rel, pl.ds(r, ROWS), :] = (
                    jnp.dot(lhs[pl.ds(k * chunk + r, ROWS), :], right, preferred_element_type=F32)
                    + pr[k, rel, pl.ds(r, ROWS), :].astype(F32)).astype(BF)
                return 0

            lax.fori_loop(0, chunk // ROWS, body, 0)
            low, high = qs.at[k, rel, pl.ds(0, half), :], qs.at[k, rel, pl.ds(half, half), :]
            ss = rr_send.at[ph, k]
            if rel == 2:
                rcopy(low, op.at[0, k], ss, rr_recv.at[ph, k, 0], to_right).start()
                rcopy(high, op.at[1, k], ss, rr_recv.at[ph, k, 1], to_left).start()
            elif rel == 1:
                rcopy(high, fi.at[0, k, pl.ds(half, half), :], ss, rr_recv.at[ph, k, 2], to_right).start()
            elif rel == 3:
                rcopy(low, fi.at[1, k, pl.ds(0, half), :], ss, rr_recv.at[ph, k, 3], to_left).start()

    def rs_c(ph, k):
        ps, pr, qs, op, fi = bufs[ph]
        ss = rr_send.at[ph, k]
        for d, rel, lo, to in ((0, 1, 0, to_right), (1, 3, half, to_left)):
            got(op.at[d, k], rr_recv.at[ph, k, d], ss, to)
            rows = pl.ds(lo, half)
            qs[k, rel, rows, :] = (qs[k, rel, rows, :].astype(F32) + op[d, k].astype(F32)).astype(BF)
            rcopy(qs.at[k, rel, rows, :], fi.at[d, k, rows, :], ss, rr_recv.at[ph, k, 4 + d], to).start()

    def rs_d(ph, k, base, put):
        ps, pr, qs, op, fi = bufs[ph]
        ss = rr_send.at[ph, k]
        got(fi.at[0, k, pl.ds(half, half), :], rr_recv.at[ph, k, 2], ss, to_right)
        got(fi.at[1, k, pl.ds(0, half), :], rr_recv.at[ph, k, 3], ss, to_left)
        got(fi.at[0, k, pl.ds(0, half), :], rr_recv.at[ph, k, 4], ss, to_right)
        got(fi.at[1, k, pl.ds(half, half), :], rr_recv.at[ph, k, 5], ss, to_left)
        for r in range(0, chunk, ROWS):
            rows = pl.ds(r, ROWS)
            total = (qs[k, 0, rows, :].astype(F32) + fi[0, k, rows, :].astype(F32)
                     + fi[1, k, rows, :].astype(F32))
            put(k * chunk + r, (base(k * chunk + r).astype(F32) + total).astype(BF))

    def column(row):
        return jnp.broadcast_to(row, (row.shape[1], row.shape[1])).T

    def joined(buf, r):
        parts = [buf[j, pl.ds(r, ROWS), :] for j in range(n_tp)]
        squares = None
        for part in parts:
            wide = part.astype(F32)
            squares = wide * wide if squares is None else squares + wide * wide
        inv = lax.rsqrt(jnp.sum(squares, axis=1, keepdims=True) / feats + EPS)
        return jnp.concatenate(parts, axis=1), inv

    def gating(k):
        for r in range(0, chunk, ROWS):
            at = k * chunk + r
            lhs, inv = joined(xg, at)
            pre = jnp.dot(lhs, wuv[...], preferred_element_type=F32) * inv * suv_ref[...]
            act = jax.nn.gelu(pre)
            ub[pl.ds(at, ROWS), :] = act[:, :u_w]
            turned = act[:, u_w:].T
            vt[:, pl.ds(at, ROWS)] = turned
            st_own[k, :, pl.ds(r, ROWS)] = jnp.concatenate(
                [jnp.sum(turned, axis=0, keepdims=True), jnp.sum(turned * turned, axis=0, keepdims=True),
                 jnp.zeros((6, ROWS), F32)], axis=0)
        rcopy(st_own.at[k], st_p.at[k], st_send.at[k], st_recv.at[k, 3], to_mate).start()

    def stats(k):
        got(st_p.at[k], st_recv.at[k, 3], st_send.at[k], to_mate)
        st_c[k] = st_own[k] + st_p[k]
        for n, to in enumerate((to_right, to_left, to_opp)):
            rcopy(st_c.at[k], st_x.at[n, k], st_send.at[k], st_recv.at[k, n], to).start()

    def mixing(k):
        for n in range(3):
            got(st_x.at[n, k], st_recv.at[k, n], st_send.at[k], to_mate)
        total = st_c[k] + st_x[0, k] + st_x[1, k] + st_x[2, k]
        mean = total[0:1] / gm_w
        square = total[1:2] / gm_w
        scale = lax.rsqrt(square - mean * mean + EPS)
        gain = column(mg_ref[...])[:, 0:1]
        for b in range(0, chunk, block):
            at = k * chunk + b
            v_norm = ((vt[:, pl.ds(at, block)] - mean[:, b:b + block]) * scale[:, b:b + block] * gain).astype(BF)
            mixed = lax.dot_general(mask[...], v_norm, (((1,), (1,)), ((), ())), preferred_element_type=F32)
            gated[pl.ds(at, block), :] = (ub[pl.ds(at, block), :] * (mixed + bias[...])).astype(BF)

    def ff_up(k):
        for r in range(0, chunk, ROWS):
            at = k * chunk + r
            lhs, inv = joined(rg, at)
            for n in range(0, h_w, 256):
                cols = pl.ds(n, 256)
                acc = jnp.dot(lhs, wup[:, n:n + 256], preferred_element_type=F32)
                acc = jnp.maximum(acc * inv * sup_ref[:, n:n + 256], 0.0)
                hid[pl.ds(at, ROWS), cols] = (acc * acc).astype(BF)

    def rounded(w):
        return w.astype(BF).astype(F32)

    own = pl.ds(pl.multiple_of(f * k_fs, k_fs), k_fs)

    tokens_at = lambda r, n: x_ref.at[pl.ds(r, n), :]
    res_at = lambda r, n: ag_rows(rg, t, r, n)
    for k in range(CHUNKS):
        ag_a(0, k, tokens_at, xg)

    g1 = column(g1_ref[pl.ds(f, 1), :])
    wuv[own, :] = (jnp.concatenate([rounded(wu_ref[...]) * g1, rounded(wv_ref[...]) * g1], axis=1)).astype(BF)
    z_hop("uv", 1)
    g2 = column(g2_ref[pl.ds(f, 1), :])[:, 0:1]
    wup[own, :] = (rounded(wup_ref[...]) * g2).astype(BF)
    A1 = ("uv", "upy", "out")
    B1 = ("upb", "dny", "dnb")
    z_hop("upy", 1)
    wout[f] = (rounded(wo_ref[...]) * so_ref[...]).astype(BF)
    z_hop("out", 1)
    xg[t] = x_ref[...]
    wdn[f] = (rounded(wdn_ref[...]) * sdn_ref[...]).astype(BF)
    low = lax.broadcasted_iota(jnp.int32, (block, block), 0) >= lax.broadcasted_iota(jnp.int32, (block, block), 1)
    grp_at = t * u_w // (gm_w // sw_ref.shape[0])
    mask[...] = jnp.where(low, sw_ref[grp_at], 0.0).astype(BF)
    bias[...] = column(sb_ref[pl.ds(grp_at, 1), :])

    def z_round(names, hop):
        for name in names:
            z_hop(name, hop)

    z_round(A1, 2)
    z_round(A1, 3)
    ag_b(0, 0, xg)
    z_round(A1, 4)
    ag_b(0, 1, xg)
    z_round(A1, 5)
    ag_c(0, 0, xg)
    z_round(A1, 6)
    ag_c(0, 1, xg)
    z_round(A1, 7)
    ag_d(0, 0, xg)
    ag_d(0, 1, xg)
    z_round(A1, 8)
    z_round(B1, 1)
    z_round(A1, 9)

    gating(0)
    gating(1)
    stats(0)
    stats(1)
    z_round(B1, 2)
    mixing(0)
    rs_a(0, 0, gated, wout)
    mixing(1)
    rs_a(0, 1, gated, wout)
    rs_b(0, 0, gated, wout)
    rs_b(0, 1, gated, wout)
    z_round(B1, 3)
    rs_c(0, 0)
    z_round(B1, 4)
    rs_c(0, 1)

    def base1(r):
        return x_ref[pl.ds(r, ROWS), :]

    def put1(r, v):
        rg[t, pl.ds(r, ROWS), :] = v

    rs_d(0, 0, base1, put1)
    ag_a(1, 0, res_at, rg)
    z_round(B1, 5)
    rs_d(0, 1, base1, put1)
    ag_a(1, 1, res_at, rg)
    z_round(B1, 6)
    ag_b(1, 0, rg)
    z_round(B1, 7)
    ag_b(1, 1, rg)
    z_round(B1, 8)
    ag_c(1, 0, rg)
    z_round(B1, 9)
    ag_c(1, 1, rg)
    y_done("upy")
    ag_d(1, 0, rg)
    ff_up(0)
    y_done("dny")
    rs_a(1, 0, hid, wdn)
    ag_d(1, 1, rg)
    rs_b(1, 0, hid, wdn)
    ff_up(1)
    rs_c(1, 0)
    rs_a(1, 1, hid, wdn)
    rs_b(1, 1, hid, wdn)

    def base2(r):
        return rg[t, pl.ds(r, ROWS), :]

    def put2(r, v):
        out_ref[pl.ds(r, ROWS), :] = v

    rs_d(1, 0, base2, put2)
    rs_c(1, 1)
    rs_d(1, 1, base2, put2)

    for s in streams.values():
        sent(s.whole, z_send.at[s.index], z_recv.at[s.index, 0, 0], to_up)
        if s.paired:
            sent(s.whole, y_send.at[s.index], y_recv.at[s.index], to_pair)
    for ph, buf in ((0, xg), (1, rg)):
        ps, pr, qs, op, fi = bufs[ph]
        for k in range(CHUNKS):
            rows = pl.ds(k * chunk, chunk)
            sent(buf.at[pl.ds(0, 3), rows, :], ag_send.at[ph, k], ag_recv.at[ph, k, 0], to_right)
            sent(buf.at[pl.ds(0, n_x), rows, :], agp_send.at[ph, k], agp_recv.at[ph, k], to_mate)
            sent(ps.at[k], rp_send.at[ph, k], rp_recv.at[ph, k, 0], to_mate)
            sent(qs.at[k, pl.ds(0, 3)], rr_send.at[ph, k], rr_recv.at[ph, k, 0], to_right)
    for k in range(CHUNKS):
        sent(st_x.at[pl.ds(0, 4), k], st_send.at[k], st_recv.at[k, 0], to_mate)


def per_device(dims, tokens, norm1_gain, weight_u, weight_v, scale_u, scale_v, mix_gain, spatial_weight,
               spatial_bias, weight_out, scale_out, norm2_gain, weight_up, scale_up, weight_down, scale_down):
    n_fs, n_tp = dims["fs"], dims["tp"]
    rows, width = tokens.shape
    feats = width * n_tp
    u_w, h_w = weight_u.shape[1], weight_up.shape[1]
    o_w, d_w = weight_out.shape[1], weight_down.shape[1]
    chunk = rows // CHUNKS
    block = spatial_weight.shape[1]
    n_x = n_tp // CORES
    if n_x != 4 or width != 2 * o_w or width != 2 * d_w:
        raise ValueError("unsupported mesh")
    args = (
        tokens, norm1_gain.reshape(n_fs, -1), weight_u, weight_v,
        jnp.concatenate([scale_u, scale_v]).reshape(1, -1), mix_gain.reshape(1, -1), spatial_weight, spatial_bias,
        weight_out, scale_out.reshape(1, -1), norm2_gain.reshape(n_fs, -1), weight_up, scale_up.reshape(1, -1),
        weight_down, scale_down.reshape(1, -1),
    )
    rs = [
        pltpu.VMEM((CHUNKS, n_x, chunk, width), BF),
        pltpu.VMEM((CHUNKS, n_x, chunk, width), BF),
        pltpu.VMEM((CHUNKS, n_x, chunk, width), BF),
        pltpu.VMEM((2, CHUNKS, chunk // 2, width), BF),
        pltpu.VMEM((2, CHUNKS, chunk, width), BF),
    ]
    dma = pltpu.SemaphoreType.DMA
    n_streams = 6
    scratch = [
        pltpu.VMEM((feats, 2 * u_w), BF),
        pltpu.VMEM((n_fs, u_w, o_w), BF),
        pltpu.VMEM((feats, h_w), BF),
        pltpu.VMEM((n_fs, h_w, d_w), BF),
        pltpu.VMEM((n_tp, rows, width), BF),
        pltpu.VMEM((n_tp, rows, width), BF),
        pltpu.VMEM((rows, u_w), F32),
        pltpu.VMEM((u_w, rows), F32),
        pltpu.VMEM((CHUNKS, 8, chunk), F32),
        pltpu.VMEM((CHUNKS, 8, chunk), F32),
        pltpu.VMEM((CHUNKS, 8, chunk), F32),
        pltpu.VMEM((4, CHUNKS, 8, chunk), F32),
        pltpu.VMEM((rows, u_w), BF),
        pltpu.VMEM((rows, h_w), BF),
        *rs, *rs,
        pltpu.VMEM((block, block), BF),
        pltpu.VMEM((block, block), F32),
        dma((n_streams, 2, n_fs // 2)), dma((n_streams,)), dma((n_streams,)), dma((n_streams,)),
        dma((2, CHUNKS, 4)), dma((2, CHUNKS)), dma((2, CHUNKS)), dma((2, CHUNKS)),
        dma((2, CHUNKS, n_x)), dma((2, CHUNKS)), dma((2, CHUNKS, 6)), dma((2, CHUNKS)),
        dma((CHUNKS, 4)), dma((CHUNKS,)),
    ]
    vmem = pl.BlockSpec(memory_space=pltpu.VMEM)
    return pl.pallas_call(
        functools.partial(kernel, dims),
        out_shape=jax.ShapeDtypeStruct(tokens.shape, tokens.dtype),
        in_specs=[vmem] * len(args),
        out_specs=vmem,
        scratch_shapes=scratch,
        name="layer",
        compiler_params=pltpu.CompilerParams(
            collective_id=0, has_side_effects=True, vmem_limit_bytes=64 * 1000 * 1000),
    )(*args)


def solution(mesh):
    placed = (
        P(("grp", "fs"), "tp"), P(), P("fs", "tp"), P("fs", "tp"), P("tp"), P("tp"), P("tp"), P(), P(),
        P("tp", "fs"), P("fs"), P(), P("fs", "tp"), P("tp"), P("tp", "fs"), P("fs"),
    )
    return jax.shard_map(
        functools.partial(per_device, dict(mesh.shape)), mesh=mesh, in_specs=placed,
        out_specs=P(("grp", "fs"), "tp"), check_vma=False)
```

```python
import functools

import jax
import jax.numpy as jnp
from jax import lax
from jax.experimental import pallas as pl
from jax.experimental.pallas import tpu as pltpu
from jax.sharding import PartitionSpec as P

BF = jnp.bfloat16
F32 = jnp.float32
MESH = pl.DeviceIdType.MESH
EPS = 1e-06
CORES = 2
CHUNKS = 2
ROWS = 256


class Stream:
    def __init__(self, name, ref, rows, whole, paired):
        self.name, self.ref, self.rows, self.whole, self.paired = name, ref, rows, whole, paired


def kernel(
    dims,
    x_ref, g1_ref, wu_ref, wv_ref, su_ref, sv_ref, mg_ref, sw_ref, sb_ref, wo_ref, so_ref,
    g2_ref, wup_ref, sup_ref, wdn_ref, sdn_ref,
    out_ref,
    wuv, wout, wup, wdn, xg, rg, ub, vt, st_own, st_p, st_c, st_x, gated, hid,
    ps1, pr1, qs1, op1, fi1, ps2, pr2, qs2, op2, fi2, mask, bias, total_e,
    z_recv, z_send, y_recv, y_send, ag_recv, ag_send, agp_recv, agp_send,
    rp_recv, rp_send, rr_recv, rr_send, st_recv, st_send,
):
    n_fs, n_tp = dims["fs"], dims["tp"]
    n_x = n_tp // CORES
    half_ring = n_fs // 2
    total_rows, width = x_ref.shape
    feats = width * n_tp
    u_w = wu_ref.shape[1]
    k_fs = wu_ref.shape[0]
    h_w = wup_ref.shape[1]
    gm_w = u_w * n_tp
    chunk = total_rows // CHUNKS
    half = chunk // 2
    block = sw_ref.shape[1]
    pair = dims["grp"] % 2 == 0

    g = lax.axis_index("grp")
    f = lax.axis_index("fs")
    t = lax.axis_index("tp")
    cx = t // CORES
    core = t % CORES
    par = g % 2

    def chip(d):
        return (cx + d) % n_x

    def tp_of(d):
        return chip(d) * CORES + core

    to_right, to_left, to_opp = {"tp": tp_of(1)}, {"tp": tp_of(n_x - 1)}, {"tp": tp_of(2)}
    to_mate = {"tp": cx * CORES + 1 - core}
    to_up, to_down = {"fs": (f + 1) % n_fs}, {"fs": (f + n_fs - 1) % n_fs}
    to_pair = {"grp": g + 1 - 2 * par}

    to_up2, to_down2 = {"fs": (f + 2) % n_fs}, {"fs": (f + n_fs - 2) % n_fs}
    neighbours = [to_right, to_left, to_opp, to_mate, to_up, to_down, to_up2, to_down2]
    if pair:
        neighbours.append(to_pair)
    barrier = pltpu.get_barrier_semaphore()
    for n in neighbours:
        pl.semaphore_signal(barrier, inc=1, device_id=n, device_id_type=MESH)
    pl.semaphore_wait(barrier, len(neighbours))

    def rcopy(src, dst, ss, rs, dev):
        return pltpu.make_async_remote_copy(
            src_ref=src, dst_ref=dst, send_sem=ss, recv_sem=rs, device_id=dev, device_id_type=MESH)

    def got(ref, sem, spare, dev):
        rcopy(ref, ref, spare, sem, dev).wait_recv()

    def sent(ref, sem, spare, dev):
        rcopy(ref, ref, sem, spare, dev).wait_send()

    def rows_2d(ref, start):
        def at(slot, rows):
            return ref.at[pl.ds(pl.multiple_of(slot * k_fs + start, 16), rows), :]
        return at

    def rows_3d(ref, start):
        def at(slot, rows):
            return ref.at[slot, pl.ds(pl.multiple_of(start, 16), rows), :]
        return at

    def whole_2d(ref, rows):
        return ref.at[pl.ds(0, (n_fs - 1) * rows), :]

    def whole_3d(ref, rows):
        return ref.at[pl.ds(0, n_fs - 1), pl.ds(0, rows), :]

    def make(name, ref, three, first, own_rows, swap):
        def at(r, start):
            return (rows_3d if three else rows_2d)(r, first + start)

        whole = whole_3d if three else whole_2d
        result = []
        if pair and swap:
            shared = own_rows - 2 * swap
            result.append(Stream(name + "y", at(ref, par * (own_rows - swap)), swap, whole(ref, swap), True))
            if shared:
                result.append(Stream(name + "b", at(ref, swap), shared, whole(ref, shared), False))
        else:
            result.append(Stream(name + "y", at(ref, 0), own_rows, whole(ref, own_rows), False))
        return result

    streams = {}
    dn_half = k_fs // 2
    for s in (make("uv", wuv, False, 0, k_fs, k_fs // 2) + make("out", wout, True, 0, u_w, u_w // 2)
              + make("up", wup, False, 0, k_fs, 32) + make("e", wdn, False, 0, dn_half, 32)
              + make("f", wdn, False, dn_half, dn_half, 16)):
        s.index = len(streams)
        streams[s.name] = s

    def z_dirs(s, hop):
        return (0, 1) if hop < half_ring else (s.index % 2,)

    def z_hop(name, hop):
        s = streams[name]
        for d in (0, 1):
            to = to_up if d == 0 else to_down
            if hop > 1 and d in z_dirs(s, hop - 1):
                back = hop - 1
                slot = (f + (n_fs - back if d == 0 else back)) % n_fs
                piece = s.ref(slot, s.rows)
                got(piece, z_recv.at[s.index, d, hop - 2], z_send.at[s.index], to)
                if s.paired:
                    rcopy(piece, piece, y_send.at[s.index], y_recv.at[s.index], to_pair).start()
            if hop <= half_ring and d in z_dirs(s, hop):
                back = hop - 1
                slot = (f + (n_fs - back if d == 0 else back)) % n_fs
                piece = s.ref(slot, s.rows)
                rcopy(piece, piece, z_send.at[s.index], z_recv.at[s.index, d, hop - 1], to).start()

    FAST = ("uvy", "outy")
    stages = half_ring // 2

    def slot_at(d, back):
        return (f + (n_fs - back if d == 0 else back)) % n_fs

    def fast_piece(s, d, back):
        return s.ref(slot_at(d, back), s.rows)

    def fast_got(s, d, back):
        got(fast_piece(s, d, back), z_recv.at[s.index, d, back - 1], z_send.at[s.index], to_up)

    def to_partner(s, piece):
        if s.paired:
            rcopy(piece, piece, y_send.at[s.index], y_recv.at[s.index], to_pair).start()

    def fast(stage):
        even = 2 * (stage - 1)
        for name in FAST:
            s = streams[name]
            for d in (0, 1):
                one, two = (to_up, to_up2) if d == 0 else (to_down, to_down2)
                if stage > 1 and d in z_dirs(s, even):
                    fast_got(s, d, even)
                    to_partner(s, fast_piece(s, d, even))
                if stage <= stages:
                    piece = fast_piece(s, d, even)
                    for step, to in ((2, two), (1, one)):
                        if d in z_dirs(s, even + step):
                            rcopy(piece, piece, z_send.at[s.index], z_recv.at[s.index, d, even + step - 1], to).start()
        if stage > 1:
            for name in FAST:
                s = streams[name]
                for d in (0, 1):
                    fast_got(s, d, even - 1)
                    to_partner(s, fast_piece(s, d, even - 1))

    def y_done(name):
        s = streams[name]
        if not s.paired:
            return
        got(s.whole, y_recv.at[s.index], y_send.at[s.index], to_pair)

    def ag_rows(buf, slot, start, rows):
        return buf.at[slot, pl.ds(start, rows), :]

    def ag_a(ph, k, src, buf):
        for n, to, lo in ((0, to_right, 0), (1, to_right, half), (2, to_left, half), (3, to_left, 0)):
            at = k * chunk + lo
            rcopy(src(at, half), ag_rows(buf, t, at, half), ag_send.at[ph, k], ag_recv.at[ph, k, n], to).start()
        at = k * chunk
        rcopy(src(at, chunk), ag_rows(buf, t, at, chunk), agp_send.at[ph, k], agp_recv.at[ph, k], to_mate).start()

    def to_other_core(ph, k, piece):
        rcopy(piece, piece, agp_send.at[ph, k], agp_recv.at[ph, k], to_mate).start()

    def ag_b(ph, k, buf):
        for n, src_chip, lo, to in ((0, n_x - 1, 0, to_right), (2, 1, half, to_left)):
            part = ag_rows(buf, tp_of(src_chip), k * chunk + lo, half)
            got(part, ag_recv.at[ph, k, n], ag_send.at[ph, k], to)
            rcopy(part, part, ag_send.at[ph, k], ag_recv.at[ph, k, 4 + n // 2], to).start()

    def ag_c(ph, k, buf):
        for n, src_chip, lo, to in ((1, n_x - 1, half, to_right), (3, 1, 0, to_left)):
            part = ag_rows(buf, tp_of(src_chip), k * chunk + lo, half)
            got(part, ag_recv.at[ph, k, n], ag_send.at[ph, k], to)
            to_other_core(ph, k, ag_rows(buf, tp_of(src_chip), k * chunk, chunk))

    def ag_e(ph, k, buf):
        for n, lo in ((4, 0), (5, half)):
            part = ag_rows(buf, tp_of(2), k * chunk + lo, half)
            got(part, ag_recv.at[ph, k, n], ag_send.at[ph, k], to_right)
            to_other_core(ph, k, part)

    def ag_d(ph, k, buf):
        got(buf.at[pl.ds(0, n_x), pl.ds(k * chunk, chunk), :], agp_recv.at[ph, k], agp_send.at[ph, k], to_mate)

    bufs = ((ps1, pr1, qs1, op1, fi1), (ps2, pr2, qs2, op2, fi2))

    def products(ph, u, c):
        k, e = u % CHUNKS, u // CHUNKS
        if ph == 0:
            left = gated[pl.ds(k * chunk, chunk), :]
            for rel in (2, 1, 3, 0):
                j = chip(rel) * CORES + c
                right = jnp.concatenate([wout[2 * j], wout[2 * j + 1]], axis=1)
                yield ((rel, jnp.dot(left, right, preferred_element_type=F32)),)
        else:
            left = hid[pl.ds(k * chunk, chunk), :]
            for rels in ((2, 1), (3, 0)):
                parts = []
                for rel in rels:
                    j = chip(rel) * CORES + c
                    for shard in (2 * j, 2 * j + 1):
                        at = pl.multiple_of(shard * k_fs + e * dn_half, dn_half)
                        parts.append(wdn[pl.ds(at, dn_half), :])
                both = lax.dot_general(left, jnp.concatenate(parts, axis=0), (((1,), (1,)), ((), ())),
                                       preferred_element_type=F32)
                yield ((rels[0], both[:, :k_fs]), (rels[1], both[:, k_fs:]))

    def rs_a(ph, u):
        ps, pr = bufs[ph][:2]
        for some in products(ph, u, 1 - core):
            for rel, value in some:
                ps[u, rel] = value.astype(BF)
                rcopy(ps.at[u, rel], pr.at[u, rel], rp_send.at[ph, u], rp_recv.at[ph, u, rel], to_mate).start()

    def rs_b(ph, u):
        ps, pr, qs, op, fi = bufs[ph]
        ss = rr_send.at[ph, u]
        for some in products(ph, u, core):
            for rel, value in some:
                got(pr.at[u, rel], rp_recv.at[ph, u, rel], rp_send.at[ph, u], to_mate)
                qs[u, rel] = (value + pr[u, rel].astype(F32)).astype(BF)
                low, high = qs.at[u, rel, pl.ds(0, half), :], qs.at[u, rel, pl.ds(half, half), :]
                if rel == 2:
                    rcopy(low, op.at[0, u], ss, rr_recv.at[ph, u, 0], to_right).start()
                    rcopy(high, op.at[1, u], ss, rr_recv.at[ph, u, 1], to_left).start()
                elif rel == 1:
                    rcopy(high, fi.at[0, u, pl.ds(half, half), :], ss, rr_recv.at[ph, u, 2], to_right).start()
                elif rel == 3:
                    rcopy(low, fi.at[1, u, pl.ds(0, half), :], ss, rr_recv.at[ph, u, 3], to_left).start()

    def rs_c(ph, u):
        ps, pr, qs, op, fi = bufs[ph]
        ss = rr_send.at[ph, u]
        for d, rel, lo, to in ((0, 1, 0, to_right), (1, 3, half, to_left)):
            got(op.at[d, u], rr_recv.at[ph, u, d], ss, to)
            rows = pl.ds(lo, half)
            qs[u, rel, rows, :] = (qs[u, rel, rows, :].astype(F32) + op[d, u].astype(F32)).astype(BF)
            rcopy(qs.at[u, rel, rows, :], fi.at[d, u, rows, :], ss, rr_recv.at[ph, u, 4 + d], to).start()

    def rs_d(ph, u, put):
        ps, pr, qs, op, fi = bufs[ph]
        ss = rr_send.at[ph, u]
        got(fi.at[0, u, pl.ds(half, half), :], rr_recv.at[ph, u, 2], ss, to_right)
        got(fi.at[1, u, pl.ds(0, half), :], rr_recv.at[ph, u, 3], ss, to_left)
        got(fi.at[0, u, pl.ds(0, half), :], rr_recv.at[ph, u, 4], ss, to_right)
        got(fi.at[1, u, pl.ds(half, half), :], rr_recv.at[ph, u, 5], ss, to_left)
        for r in range(0, chunk, ROWS):
            rows = pl.ds(r, ROWS)
            put((u % CHUNKS) * chunk + r, qs[u, 0, rows, :].astype(F32) + fi[0, u, rows, :].astype(F32)
                + fi[1, u, rows, :].astype(F32))

    def column(row):
        return jnp.broadcast_to(row, (row.shape[1], row.shape[1])).T

    def joined(buf, r):
        parts = [buf[j, pl.ds(r, ROWS), :] for j in range(n_tp)]
        squares = None
        for part in parts:
            wide = part.astype(F32)
            squares = wide * wide if squares is None else squares + wide * wide
        inv = lax.rsqrt(jnp.sum(squares, axis=1, keepdims=True) / feats + EPS)
        return jnp.concatenate(parts, axis=1), inv

    def gating(k):
        scale_uv = jnp.concatenate([su_ref[...], sv_ref[...]], axis=1)
        for r in range(0, chunk, ROWS):
            at = k * chunk + r
            lhs, inv = joined(xg, at)
            pre = jnp.dot(lhs, wuv[...], preferred_element_type=F32) * inv * scale_uv
            act = jax.nn.gelu(pre)
            ub[pl.ds(at, ROWS), :] = act[:, :u_w]
            turned = act[:, u_w:].T
            vt[:, pl.ds(at, ROWS)] = turned
            st_own[k, :, pl.ds(r, ROWS)] = jnp.concatenate(
                [jnp.sum(turned, axis=0, keepdims=True), jnp.sum(turned * turned, axis=0, keepdims=True),
                 jnp.zeros((6, ROWS), F32)], axis=0)
        rcopy(st_own.at[k], st_p.at[k], st_send.at[k], st_recv.at[k, 3], to_mate).start()

    def stats(k):
        got(st_p.at[k], st_recv.at[k, 3], st_send.at[k], to_mate)
        st_c[k] = st_own[k] + st_p[k]
        for n, to in enumerate((to_right, to_left, to_opp)):
            rcopy(st_c.at[k], st_x.at[n, k], st_send.at[k], st_recv.at[k, n], to).start()

    def mixing(k):
        for n in range(3):
            got(st_x.at[n, k], st_recv.at[k, n], st_send.at[k], to_mate)
        total = st_c[k] + st_x[0, k] + st_x[1, k] + st_x[2, k]
        mean = total[0:1] / gm_w
        square = total[1:2] / gm_w
        scale = lax.rsqrt(square - mean * mean + EPS)
        gain = column(mg_ref[...])[:, 0:1]
        for b in range(0, chunk, block):
            at = k * chunk + b
            v_norm = ((vt[:, pl.ds(at, block)] - mean[:, b:b + block]) * scale[:, b:b + block] * gain).astype(BF)
            mixed = lax.dot_general(mask[...], v_norm, (((1,), (1,)), ((), ())), preferred_element_type=F32)
            gated[pl.ds(at, block), :] = (ub[pl.ds(at, block), :] * (mixed + bias[...])).astype(BF)

    def ff_up(k):
        for r in range(0, chunk, ROWS):
            at = k * chunk + r
            lhs, inv = joined(rg, at)
            for n in range(0, h_w, 256):
                cols = pl.ds(n, 256)
                acc = jnp.dot(lhs, wup[:, n:n + 256], preferred_element_type=F32)
                acc = jnp.maximum(acc * inv * sup_ref[:, n:n + 256], 0.0)
                hid[pl.ds(at, ROWS), cols] = (acc * acc).astype(BF)

    def rounded(w):
        return w.astype(BF).astype(F32)

    own = pl.ds(pl.multiple_of(f * k_fs, k_fs), k_fs)

    tokens_at = lambda r, n: x_ref.at[pl.ds(r, n), :]
    res_at = lambda r, n: ag_rows(rg, t, r, n)
    for k in range(CHUNKS):
        ag_a(0, k, tokens_at, xg)

    g1 = column(g1_ref[pl.ds(f, 1), :])
    wuv[own, :] = (jnp.concatenate([rounded(wu_ref[...]) * g1, rounded(wv_ref[...]) * g1], axis=1)).astype(BF)
    wout[f] = (rounded(wo_ref[...]) * so_ref[...]).astype(BF)
    fast(1)
    g2 = column(g2_ref[pl.ds(f, 1), :])[:, 0:1]
    wup[own, :] = (rounded(wup_ref[...]) * g2).astype(BF)
    z_hop("upb", 1)
    wdn[own, :] = (rounded(wdn_ref[...]) * sdn_ref[...]).T.astype(BF)
    xg[t] = x_ref[...]
    low = lax.broadcasted_iota(jnp.int32, (block, block), 0) >= lax.broadcasted_iota(jnp.int32, (block, block), 1)
    grp_at = t * u_w // (gm_w // sw_ref.shape[0])
    mask[...] = jnp.where(low, sw_ref[grp_at], 0.0).astype(BF)
    bias[...] = column(sb_ref[pl.ds(grp_at, 1), :])

    def z_round(*pairs):
        for name, hop in pairs:
            z_hop(name, hop)

    fast(2)
    z_hop("upb", 2)
    ag_b(0, 0, xg)
    fast(3)
    z_hop("upb", 3)
    ag_b(0, 1, xg)
    ag_c(0, 0, xg)
    fast(4)
    z_hop("upb", 4)
    ag_c(0, 1, xg)
    ag_e(0, 0, xg)
    fast(5)
    z_round(("upb", 5), ("upy", 1))
    ag_e(0, 1, xg)
    y_done("uvy")
    ag_d(0, 0, xg)
    gating(0)
    ag_d(0, 1, xg)
    gating(1)
    stats(0)
    stats(1)
    z_round(("upb", 6), ("upy", 2))
    y_done("outy")
    mixing(0)
    rs_a(0, 0)
    mixing(1)
    rs_b(0, 0)
    rs_a(0, 1)
    z_round(("upb", 7), ("upy", 3), ("ey", 1))
    rs_c(0, 0)
    rs_b(0, 1)
    z_round(("upb", 8), ("upy", 4), ("ey", 2))

    def put1(r, v):
        rg[t, pl.ds(r, ROWS), :] = (x_ref[pl.ds(r, ROWS), :].astype(F32) + v).astype(BF)

    rs_d(0, 0, put1)
    ag_a(1, 0, res_at, rg)
    rs_c(0, 1)
    z_round(("upb", 9), ("upy", 5), ("ey", 3), ("fy", 1), ("fb", 1))
    rs_d(0, 1, put1)
    ag_b(1, 0, rg)
    ag_a(1, 1, res_at, rg)
    z_round(("upy", 6), ("ey", 4), ("fy", 2), ("fb", 2))
    ag_c(1, 0, rg)
    z_round(("upy", 7), ("ey", 5), ("fy", 3), ("fb", 3))
    ag_e(1, 0, rg)
    ag_b(1, 1, rg)
    z_round(("upy", 8), ("ey", 6), ("fy", 4), ("fb", 4))
    ag_c(1, 1, rg)
    ag_d(1, 0, rg)
    z_round(("upy", 9), ("ey", 7), ("fy", 5), ("fb", 5))
    ag_e(1, 1, rg)
    y_done("upy")
    ff_up(0)
    z_round(("ey", 8), ("fy", 6), ("fb", 6))
    ag_d(1, 1, rg)
    ff_up(1)
    z_round(("ey", 9), ("fy", 7), ("fb", 7))
    y_done("ey")
    rs_a(1, 0)
    rs_b(1, 0)
    z_round(("fy", 8), ("fb", 8))
    rs_a(1, 1)
    rs_c(1, 0)
    rs_b(1, 1)
    z_round(("fy", 9), ("fb", 9))
    rs_c(1, 1)
    y_done("fy")
    rs_a(1, 2)
    rs_b(1, 2)

    def put_e(r, v):
        total_e[pl.ds(r, ROWS), :] = v

    def put2(r, v):
        rows = pl.ds(r, ROWS)
        first, h = total_e[rows, :], dn_half
        total = jnp.concatenate([first[:, :h], v[:, :h], first[:, h:], v[:, h:]], axis=1)
        out_ref[rows, :] = (rg[t, rows, :].astype(F32) + total).astype(BF)

    rs_a(1, 3)
    rs_d(1, 0, put_e)
    rs_c(1, 2)
    rs_b(1, 3)
    rs_d(1, 1, put_e)
    rs_c(1, 3)
    rs_d(1, 2, put2)
    rs_d(1, 3, put2)

    for s in streams.values():
        sent(s.whole, z_send.at[s.index], z_recv.at[s.index, 0, 0], to_up)
        if s.paired:
            sent(s.whole, y_send.at[s.index], y_recv.at[s.index], to_pair)
    for ph, buf in ((0, xg), (1, rg)):
        ps, pr, qs, op, fi = bufs[ph]
        for k in range(CHUNKS):
            rows = pl.ds(k * chunk, chunk)
            sent(buf.at[pl.ds(0, 3), rows, :], ag_send.at[ph, k], ag_recv.at[ph, k, 0], to_right)
            sent(buf.at[pl.ds(0, n_x), rows, :], agp_send.at[ph, k], agp_recv.at[ph, k], to_mate)
        for u in range(CHUNKS * (1 + ph)):
            sent(ps.at[u], rp_send.at[ph, u], rp_recv.at[ph, u, 0], to_mate)
            sent(qs.at[u, pl.ds(0, 3)], rr_send.at[ph, u], rr_recv.at[ph, u, 0], to_right)
    for k in range(CHUNKS):
        sent(st_x.at[pl.ds(0, 4), k], st_send.at[k], st_recv.at[k, 0], to_mate)


def per_device(dims, tokens, norm1_gain, weight_u, weight_v, scale_u, scale_v, mix_gain, spatial_weight,
               spatial_bias, weight_out, scale_out, norm2_gain, weight_up, scale_up, weight_down, scale_down):
    n_fs, n_tp = dims["fs"], dims["tp"]
    rows, width = tokens.shape
    feats = width * n_tp
    u_w, h_w = weight_u.shape[1], weight_up.shape[1]
    o_w, d_w = weight_out.shape[1], weight_down.shape[1]
    chunk = rows // CHUNKS
    block = spatial_weight.shape[1]
    n_x = n_tp // CORES
    if n_x != 4 or width != 2 * o_w or width != 2 * d_w:
        raise ValueError("unsupported mesh")
    args = (
        tokens, norm1_gain.reshape(n_fs, -1), weight_u, weight_v,
        scale_u.reshape(1, -1), scale_v.reshape(1, -1), mix_gain.reshape(1, -1), spatial_weight, spatial_bias,
        weight_out, scale_out.reshape(1, -1), norm2_gain.reshape(n_fs, -1), weight_up, scale_up.reshape(1, -1),
        weight_down, scale_down.reshape(1, -1),
    )
    def rs(units, cols):
        return [
            pltpu.VMEM((units, n_x, chunk, cols), BF),
            pltpu.VMEM((units, n_x, chunk, cols), BF),
            pltpu.VMEM((units, n_x, chunk, cols), BF),
            pltpu.VMEM((2, units, chunk // 2, cols), BF),
            pltpu.VMEM((2, units, chunk, cols), BF),
        ]

    dma = pltpu.SemaphoreType.DMA
    n_streams, units = 8, 2 * CHUNKS
    scratch = [
        pltpu.VMEM((feats, 2 * u_w), BF),
        pltpu.VMEM((n_fs, u_w, o_w), BF),
        pltpu.VMEM((feats, h_w), BF),
        pltpu.VMEM((feats, h_w), BF),
        pltpu.VMEM((n_tp, rows, width), BF),
        pltpu.VMEM((n_tp, rows, width), BF),
        pltpu.VMEM((rows, u_w), F32),
        pltpu.VMEM((u_w, rows), F32),
        pltpu.VMEM((CHUNKS, 8, chunk), F32),
        pltpu.VMEM((CHUNKS, 8, chunk), F32),
        pltpu.VMEM((CHUNKS, 8, chunk), F32),
        pltpu.VMEM((4, CHUNKS, 8, chunk), F32),
        pltpu.VMEM((rows, u_w), BF),
        pltpu.VMEM((rows, h_w), BF),
        *rs(CHUNKS, width), *rs(2 * CHUNKS, d_w),
        pltpu.VMEM((block, block), BF),
        pltpu.VMEM((block, block), F32),
        pltpu.VMEM((rows, d_w), F32),
        dma((n_streams, 2, n_fs // 2)), dma((n_streams,)), dma((n_streams,)), dma((n_streams,)),
        dma((2, CHUNKS, 6)), dma((2, CHUNKS)), dma((2, CHUNKS)), dma((2, CHUNKS)),
        dma((2, units, n_x)), dma((2, units)), dma((2, units, 6)), dma((2, units)),
        dma((CHUNKS, 4)), dma((CHUNKS,)),
    ]
    vmem = pl.BlockSpec(memory_space=pltpu.VMEM)
    return pl.pallas_call(
        functools.partial(kernel, dims),
        out_shape=jax.ShapeDtypeStruct(tokens.shape, tokens.dtype),
        in_specs=[vmem] * len(args),
        out_specs=vmem,
        scratch_shapes=scratch,
        name="layer",
        compiler_params=pltpu.CompilerParams(
            collective_id=0, has_side_effects=True, vmem_limit_bytes=64 * 1000 * 1000),
    )(*args)


def solution(mesh):
    placed = (
        P(("grp", "fs"), "tp"), P(), P("fs", "tp"), P("fs", "tp"), P("tp"), P("tp"), P("tp"), P(), P(),
        P("tp", "fs"), P("fs"), P(), P("fs", "tp"), P("tp"), P("tp", "fs"), P("fs"),
    )
    return jax.shard_map(
        functools.partial(per_device, dict(mesh.shape)), mesh=mesh, in_specs=placed,
        out_specs=P(("grp", "fs"), "tp"), check_vma=False)
```

```python
import functools

import jax
import jax.numpy as jnp
from jax import lax
from jax.experimental import pallas as pl
from jax.experimental.pallas import tpu as pltpu
from jax.sharding import PartitionSpec as P

BF = jnp.bfloat16
F32 = jnp.float32
MESH = pl.DeviceIdType.MESH
EPS = 1e-06
CORES = 2
CHUNKS = 2
ROWS = 256
SWAP = {"uv": 64, "out": 64, "up": 32, "dn": 384}
ORDER = (
    ("prep", 0), ("fe", "uvy", 1, 0), ("fe", "outy", 1, 1), ("prep", 1), ("aga", 0, 1), ("fe", "uvy", 1, 1),
    ("prep", 2), ("z", "upy", 1, 0), ("z", "upy", 1, 1), ("fo", "outy", 2, 1), ("fe", "outy", 1, 0),
    ("fe", "outy", 2, 1), ("fe", "uvy", 2, 0), ("aga", 0, 0), ("fo", "uvy", 2, 0), ("fe", "uvy", 2, 1),
    ("z", "upy", 2, 0), ("z", "upy", 2, 1), ("agb", 0, 1, 0), ("fe", "outy", 2, 0), ("fo", "uvy", 2, 1),
    ("fe", "uvy", 3, 0), ("z", "dny", 1, 0), ("fe", "outy", 3, 1), ("z", "dnb", 1, 1), ("fe", "uvy", 3, 1),
    ("fo", "uvy", 3, 1), ("agb", 0, 0, 1), ("fo", "uvy", 3, 0), ("z", "upy", 3, 1), ("z", "upy", 3, 0),
    ("z", "dny", 1, 1), ("agb", 0, 0, 0), ("fe", "uvy", 4, 0), ("fo", "outy", 2, 0), ("agb", 0, 1, 1),
    ("fo", "uvy", 4, 1), ("fo", "outy", 3, 1), ("fe", "outy", 3, 0), ("fe", "uvy", 4, 1), ("z", "dnb", 1, 0),
    ("fo", "uvy", 4, 0), ("z", "dny", 2, 0), ("z", "upb", 1, 1), ("fe", "uvy", 5, 0), ("fo", "outy", 3, 0),
    ("age", 0, 1, 0), ("agc", 0, 1, 1), ("agc", 0, 0, 1), ("fo", "uvy", 5, 0), ("fo", "uvy", 5, 1),
    ("fo", "outy", 4, 1), ("fe", "outy", 4, 0), ("agc", 0, 0, 0), ("age", 0, 0, 1), ("z", "dnb", 2, 1),
    ("agc", 0, 1, 0), ("z", "upb", 1, 0), ("fe", "uvy", 5, 1), ("age", 0, 1, 1), ("fo", "outy", 4, 0),
    ("z", "dny", 2, 1), ("fe", "outy", 4, 1), ("z", "upb", 2, 1), ("age", 0, 0, 0), ("z", "dnb", 2, 0),
    ("z", "upy", 4, 0), ("fo", "outy", 5, 0), ("z", "upy", 4, 1), ("agd", 0, 0), ("z", "dnb", 3, 1),
    ("z", "dny", 3, 0), ("yd", "uvy"), ("gating", 0), ("stats", 0), ("z", "upy", 5, 0), ("z", "upb", 2, 0),
    ("z", "upb", 3, 1), ("z", "dny", 3, 1), ("agd", 0, 1), ("gating", 1), ("fo", "outy", 5, 1), ("z", "dny", 4, 0),
    ("fe", "outy", 5, 0), ("z", "dnb", 3, 0), ("z", "upy", 5, 1), ("stats", 1), ("mixing", 0), ("aga", 2, 0),
    ("fe", "outy", 5, 1), ("z", "dnb", 4, 1), ("z", "upb", 3, 0), ("z", "upy", 6, 0), ("z", "upb", 4, 1),
    ("mixing", 1), ("aga", 2, 1), ("z", "upy", 6, 1), ("z", "dny", 5, 0), ("yd", "outy"), ("z", "dnb", 4, 0),
    ("z", "dny", 4, 1), ("z", "upy", 7, 0), ("agb", 2, 0, 1), ("agb", 2, 1, 0), ("a2s",), ("agc", 2, 0, 1),
    ("agb", 2, 1, 1), ("z", "upb", 5, 1), ("agb", 2, 0, 0), ("z", "upb", 4, 0), ("agc", 2, 1, 1), ("z", "upy", 7, 1),
    ("z", "dnb", 5, 1), ("z", "dnb", 5, 0), ("z", "upy", 8, 0), ("z", "dny", 6, 0), ("agc", 2, 0, 0),
    ("z", "dny", 5, 1), ("age", 2, 1, 0), ("z", "upb", 6, 1), ("z", "upb", 5, 0), ("age", 2, 1, 1), ("a2w",),
    ("agc", 2, 1, 0), ("z", "dnb", 6, 0), ("z", "dny", 6, 1), ("z", "dny", 7, 0), ("z", "dnb", 6, 1), ("agd", 2, 1),
    ("z", "upy", 9, 0), ("outp", 1), ("age", 2, 0, 1), ("aga", 1, 1), ("z", "upb", 7, 1), ("z", "upb", 6, 0),
    ("z", "dny", 7, 1), ("age", 2, 0, 0), ("z", "upy", 8, 1), ("z", "dny", 8, 0), ("z", "dnb", 7, 1), ("agd", 2, 0),
    ("agb", 1, 1, 1), ("agb", 1, 1, 0), ("z", "upb", 7, 0), ("outp", 0), ("z", "upb", 8, 1), ("agc", 1, 1, 1),
    ("agc", 1, 1, 0), ("aga", 1, 0), ("z", "dny", 9, 0), ("age", 1, 1, 0), ("z", "dny", 8, 1), ("z", "dnb", 7, 0),
    ("z", "dnb", 8, 1), ("age", 1, 1, 1), ("agd", 1, 1), ("yd", "upy"), ("z", "upb", 9, 1), ("agb", 1, 0, 1),
    ("agb", 1, 0, 0), ("z", "upb", 8, 0), ("ffup", 1), ("z", "dnb", 8, 0), ("z", "dnb", 9, 1), ("yd", "dny"),
    ("rsa", 1, 0), ("rsa", 1, 1), ("rsb", 1, 0), ("age", 1, 0, 1), ("agc", 1, 0, 1), ("agc", 1, 0, 0),
    ("age", 1, 0, 0), ("rsb", 1, 1), ("agd", 1, 0), ("ffup", 0), ("rsc", 1, 0), ("rsc", 1, 1), ("rsa", 0, 0),
    ("rsa", 0, 1), ("rsb", 0, 0), ("rsb", 0, 1), ("rsd", 1), ("rsc", 0, 1), ("rsc", 0, 0), ("rsd", 0),
)


class Stream:
    def __init__(self, name, ref, rows, whole, paired):
        self.name, self.ref, self.rows, self.whole, self.paired = name, ref, rows, whole, paired


def kernel(
    dims,
    x_ref, g1_ref, wu_ref, wv_ref, su_ref, sv_ref, mg_ref, sw_ref, sb_ref, wo_ref, so_ref,
    g2_ref, wup_ref, sup_ref, wdn_ref, sdn_ref,
    out_ref,
    wuv, wout, wup, wdn, xg, rg, gg, wmix, ub, vt, st_own, st_p, st_c, st_x, hid,
    ps, pr, qs, op, fi, mask, bias,
    z_recv, z_send, y_recv, y_send, ag_recv, ag_send, agp_recv, agp_send,
    rp_recv, rp_send, rr_recv, rr_send, st_recv, st_send, a2_recv, a2_send,
):
    n_fs, n_tp = dims["fs"], dims["tp"]
    n_x = n_tp // CORES
    half_ring = n_fs // 2
    total_rows, width = x_ref.shape
    feats = width * n_tp
    u_w = wu_ref.shape[1]
    k_fs = wu_ref.shape[0]
    h_w = wup_ref.shape[1]
    gm_w = u_w * n_tp
    chunk = total_rows // CHUNKS
    half = chunk // 2
    block = sw_ref.shape[1]
    pair = dims["grp"] % 2 == 0

    g = lax.axis_index("grp")
    f = lax.axis_index("fs")
    t = lax.axis_index("tp")
    cx = t // CORES
    core = t % CORES
    par = g % 2

    def chip(d):
        return (cx + d) % n_x

    def tp_of(d):
        return chip(d) * CORES + core

    to_right, to_left, to_opp = {"tp": tp_of(1)}, {"tp": tp_of(n_x - 1)}, {"tp": tp_of(2)}
    to_mate = {"tp": cx * CORES + 1 - core}
    to_up, to_down = {"fs": (f + 1) % n_fs}, {"fs": (f + n_fs - 1) % n_fs}
    to_pair = {"grp": g + 1 - 2 * par}

    to_up2, to_down2 = {"fs": (f + 2) % n_fs}, {"fs": (f + n_fs - 2) % n_fs}
    others = [{"tp": chip(rel) * CORES + (core + c) % CORES} for rel in range(n_x) for c in range(CORES) if rel or c]
    neighbours = others + [to_up, to_down, to_up2, to_down2]
    if pair:
        neighbours.append(to_pair)
    barrier = pltpu.get_barrier_semaphore()
    for n in neighbours:
        pl.semaphore_signal(barrier, inc=1, device_id=n, device_id_type=MESH)
    pl.semaphore_wait(barrier, len(neighbours))

    def rcopy(src, dst, ss, rs, dev):
        return pltpu.make_async_remote_copy(
            src_ref=src, dst_ref=dst, send_sem=ss, recv_sem=rs, device_id=dev, device_id_type=MESH)

    def got(ref, sem, spare, dev):
        rcopy(ref, ref, spare, sem, dev).wait_recv()

    def sent(ref, sem, spare, dev):
        rcopy(ref, ref, sem, spare, dev).wait_send()

    def rows_2d(ref, start):
        def at(slot, rows):
            return ref.at[pl.ds(pl.multiple_of(slot * k_fs + start, 16), rows), :]
        return at

    def rows_3d(ref, start):
        def at(slot, rows):
            return ref.at[slot, pl.ds(pl.multiple_of(start, 16), rows), :]
        return at

    def whole_2d(ref, rows):
        return ref.at[pl.ds(0, (n_fs - 1) * rows), :]

    def whole_3d(ref, rows):
        return ref.at[pl.ds(0, n_fs - 1), pl.ds(0, rows), :]

    def make(name, ref, three, first, own_rows, swap):
        def at(r, start):
            return (rows_3d if three else rows_2d)(r, first + start)

        whole = whole_3d if three else whole_2d
        result = []
        if pair and swap:
            shared = own_rows - 2 * swap
            result.append(Stream(name + "y", at(ref, par * (own_rows - swap)), swap, whole(ref, swap), True))
            if shared:
                result.append(Stream(name + "b", at(ref, swap), shared, whole(ref, shared), False))
        else:
            result.append(Stream(name + "y", at(ref, 0), own_rows, whole(ref, own_rows), False))
        return result

    streams = {}
    for s in (make("uv", wuv, False, 0, k_fs, SWAP["uv"]) + make("out", wout, True, 0, u_w, SWAP["out"])
              + make("up", wup, False, 0, k_fs, SWAP["up"]) + make("dn", wdn, True, 0, h_w, SWAP["dn"])):
        s.index = len(streams)
        streams[s.name] = s

    def z_dirs(s, hop):
        return (0, 1) if hop < half_ring else (s.index % 2,)

    def piece_at(s, d, back):
        return s.ref((f + (n_fs - back if d == 0 else back)) % n_fs, s.rows)

    def z_got(s, d, hop):
        piece = piece_at(s, d, hop)
        got(piece, z_recv.at[s.index, d, hop - 1], z_send.at[s.index], to_up)
        return piece

    def z_send_on(s, d, back, hop, to):
        piece = piece_at(s, d, back)
        rcopy(piece, piece, z_send.at[s.index], z_recv.at[s.index, d, hop - 1], to).start()

    def to_partner(s, piece):
        if s.paired:
            rcopy(piece, piece, y_send.at[s.index], y_recv.at[s.index], to_pair).start()

    def z_hop(name, hop, d):
        s = streams[name]
        if hop > 1 and d in z_dirs(s, hop - 1):
            to_partner(s, z_got(s, d, hop - 1))
        if hop <= half_ring and d in z_dirs(s, hop):
            z_send_on(s, d, hop - 1, hop, to_down if d else to_up)

    def z_even(name, stage, d):
        s = streams[name]
        even = 2 * (stage - 1)
        arrived = stage > 1 and d in z_dirs(s, even)
        if arrived:
            piece = z_got(s, d, even)
        if even < half_ring:
            for step, to in ((2, to_down2 if d else to_up2), (1, to_down if d else to_up)):
                if d in z_dirs(s, even + step):
                    z_send_on(s, d, even, even + step, to)
        if arrived:
            to_partner(s, piece)

    def z_odd(name, stage, d):
        s = streams[name]
        to_partner(s, z_got(s, d, 2 * stage - 3))

    def y_done(name):
        s = streams[name]
        if not s.paired:
            return
        got(s.whole, y_recv.at[s.index], y_send.at[s.index], to_pair)

    def ag_rows(buf, slot, start, rows):
        return buf.at[slot, pl.ds(start, rows), :]

    gathered = (xg, rg, gg)

    def to_other_core(ph, k, piece):
        rcopy(piece, piece, agp_send.at[ph, k], agp_recv.at[ph, k], to_mate).start()

    def ag_a(ph, k):
        buf = gathered[ph]

        def src(at, n):
            return x_ref.at[pl.ds(at, n), :] if ph == 0 else ag_rows(buf, t, at, n)

        for n, to, lo in ((0, to_right, 0), (1, to_right, half), (2, to_left, half), (3, to_left, 0)):
            at = k * chunk + lo
            rcopy(src(at, half), ag_rows(buf, t, at, half), ag_send.at[ph, k], ag_recv.at[ph, k, n], to).start()
        at = k * chunk
        rcopy(src(at, chunk), ag_rows(buf, t, at, chunk), agp_send.at[ph, k], agp_recv.at[ph, k], to_mate).start()

    SIDES = ((n_x - 1, 0, to_right), (1, half, to_left))

    def ag_b(ph, k, side):
        chip_at, lo, to = SIDES[side]
        part = ag_rows(gathered[ph], tp_of(chip_at), k * chunk + lo, half)
        got(part, ag_recv.at[ph, k, 2 * side], ag_send.at[ph, k], to)
        rcopy(part, part, ag_send.at[ph, k], ag_recv.at[ph, k, 4 + side], to).start()

    def ag_c(ph, k, side):
        chip_at, lo, to = SIDES[side]
        part = ag_rows(gathered[ph], tp_of(chip_at), k * chunk + half - lo, half)
        got(part, ag_recv.at[ph, k, 2 * side + 1], ag_send.at[ph, k], to)
        to_other_core(ph, k, ag_rows(gathered[ph], tp_of(chip_at), k * chunk, chunk))

    def ag_e(ph, k, side):
        part = ag_rows(gathered[ph], tp_of(2), k * chunk + SIDES[side][1], half)
        got(part, ag_recv.at[ph, k, 4 + side], ag_send.at[ph, k], to_right)
        to_other_core(ph, k, part)

    def ag_d(ph, k):
        got(gathered[ph].at[pl.ds(0, n_x), pl.ds(k * chunk, chunk), :], agp_recv.at[ph, k], agp_send.at[ph, k], to_mate)

    def a2_s():
        for n, to in enumerate(others):
            rcopy(wout.at[pl.ds(2 * to["tp"], 2)], wmix.at[t], a2_send.at[0], a2_recv.at[0], to).start()
        wmix[t] = wout[pl.ds(2 * t, 2)]

    def a2_w():
        got(wmix.at[pl.ds(0, n_tp - 1)], a2_recv.at[0], a2_send.at[0], to_mate)

    def out_p(k):
        rows = pl.ds(k * chunk, chunk)
        left = jnp.concatenate([gg[j, rows, :] for j in range(n_tp)], axis=1)
        right = jnp.concatenate(
            [jnp.concatenate([wmix[j, 0], wmix[j, 1]], axis=1) for j in range(n_tp)], axis=0)
        total = jnp.dot(left, right, preferred_element_type=F32)
        rg[t, rows, :] = (x_ref[rows, :].astype(F32) + total).astype(BF)

    PAIRS = ((2, 1), (3, 0))

    def product(k, rel, c):
        j = chip(rel) * CORES + c
        right = jnp.concatenate([wdn[2 * j], wdn[2 * j + 1]], axis=1)
        return jnp.dot(hid[pl.ds(k * chunk, chunk), :], right, preferred_element_type=F32)

    def rs_a(k, p):
        for rel in PAIRS[p]:
            ps[k, rel] = product(k, rel, 1 - core).astype(BF)
            rcopy(ps.at[k, rel], pr.at[k, rel], rp_send.at[k], rp_recv.at[k, rel], to_mate).start()

    def rs_b(k, p):
        ss = rr_send.at[k]
        for rel in PAIRS[p]:
            got(pr.at[k, rel], rp_recv.at[k, rel], rp_send.at[k], to_mate)
            qs[k, rel] = (product(k, rel, core) + pr[k, rel].astype(F32)).astype(BF)
            low, high = qs.at[k, rel, pl.ds(0, half), :], qs.at[k, rel, pl.ds(half, half), :]
            if rel == 2:
                rcopy(low, op.at[0, k], ss, rr_recv.at[k, 0], to_right).start()
                rcopy(high, op.at[1, k], ss, rr_recv.at[k, 1], to_left).start()
            elif rel == 1:
                rcopy(high, fi.at[0, k, pl.ds(half, half), :], ss, rr_recv.at[k, 2], to_right).start()
            elif rel == 3:
                rcopy(low, fi.at[1, k, pl.ds(0, half), :], ss, rr_recv.at[k, 3], to_left).start()

    def rs_c(k, side):
        ss = rr_send.at[k]
        rel, (_, lo, to) = (1, 3)[side], SIDES[side]
        got(op.at[side, k], rr_recv.at[k, side], ss, to)
        rows = pl.ds(lo, half)
        qs[k, rel, rows, :] = (qs[k, rel, rows, :].astype(F32) + op[side, k].astype(F32)).astype(BF)
        rcopy(qs.at[k, rel, rows, :], fi.at[side, k, rows, :], ss, rr_recv.at[k, 4 + side], to).start()

    def rs_d(k):
        ss = rr_send.at[k]
        for n, side, lo in ((2, 0, half), (3, 1, 0), (4, 0, 0), (5, 1, half)):
            got(fi.at[side, k, pl.ds(lo, half), :], rr_recv.at[k, n], ss, to_right)
        for r in range(0, chunk, ROWS):
            rows, at = pl.ds(r, ROWS), pl.ds(k * chunk + r, ROWS)
            total = qs[k, 0, rows, :].astype(F32) + fi[0, k, rows, :].astype(F32) + fi[1, k, rows, :].astype(F32)
            out_ref[at, :] = (rg[t, at, :].astype(F32) + total).astype(BF)

    def column(row):
        return jnp.broadcast_to(row, (row.shape[1], row.shape[1])).T

    def joined(buf, r):
        parts = [buf[j, pl.ds(r, ROWS), :] for j in range(n_tp)]
        squares = None
        for part in parts:
            wide = part.astype(F32)
            squares = wide * wide if squares is None else squares + wide * wide
        inv = lax.rsqrt(jnp.sum(squares, axis=1, keepdims=True) / feats + EPS)
        return jnp.concatenate(parts, axis=1), inv

    def gating(k):
        scale_uv = jnp.concatenate([su_ref[...], sv_ref[...]], axis=1)
        for r in range(0, chunk, ROWS):
            at = k * chunk + r
            lhs, inv = joined(xg, at)
            pre = jnp.dot(lhs, wuv[...], preferred_element_type=F32) * inv * scale_uv
            act = jax.nn.gelu(pre)
            ub[pl.ds(at, ROWS), :] = act[:, :u_w]
            turned = act[:, u_w:].T
            vt[:, pl.ds(at, ROWS)] = turned
            st_own[k, :, pl.ds(r, ROWS)] = jnp.concatenate(
                [jnp.sum(turned, axis=0, keepdims=True), jnp.sum(turned * turned, axis=0, keepdims=True),
                 jnp.zeros((6, ROWS), F32)], axis=0)
        rcopy(st_own.at[k], st_p.at[k], st_send.at[k], st_recv.at[k, 3], to_mate).start()

    def stats(k):
        got(st_p.at[k], st_recv.at[k, 3], st_send.at[k], to_mate)
        st_c[k] = st_own[k] + st_p[k]
        for n, to in enumerate((to_right, to_left, to_opp)):
            rcopy(st_c.at[k], st_x.at[n, k], st_send.at[k], st_recv.at[k, n], to).start()

    def mixing(k):
        for n in range(3):
            got(st_x.at[n, k], st_recv.at[k, n], st_send.at[k], to_mate)
        total = st_c[k] + st_x[0, k] + st_x[1, k] + st_x[2, k]
        mean = total[0:1] / gm_w
        square = total[1:2] / gm_w
        scale = lax.rsqrt(square - mean * mean + EPS)
        gain = column(mg_ref[...])[:, 0:1]
        for b in range(0, chunk, block):
            at = k * chunk + b
            v_norm = ((vt[:, pl.ds(at, block)] - mean[:, b:b + block]) * scale[:, b:b + block] * gain).astype(BF)
            mixed = lax.dot_general(mask[...], v_norm, (((1,), (1,)), ((), ())), preferred_element_type=F32)
            gg[t, pl.ds(at, block), :] = (ub[pl.ds(at, block), :] * (mixed + bias[...])).astype(BF)

    def ff_up(k):
        for r in range(0, chunk, ROWS):
            at = k * chunk + r
            lhs, inv = joined(rg, at)
            for n in range(0, h_w, 256):
                cols = pl.ds(n, 256)
                acc = jnp.dot(lhs, wup[:, n:n + 256], preferred_element_type=F32)
                acc = jnp.maximum(acc * inv * sup_ref[:, n:n + 256], 0.0)
                hid[pl.ds(at, ROWS), cols] = (acc * acc).astype(BF)

    def rounded(w):
        return w.astype(BF).astype(F32)

    own = pl.ds(pl.multiple_of(f * k_fs, k_fs), k_fs)

    def prep(n):
        if n == 0:
            g1 = column(g1_ref[pl.ds(f, 1), :])
            wuv[own, :] = (jnp.concatenate([rounded(wu_ref[...]) * g1, rounded(wv_ref[...]) * g1], axis=1)).astype(BF)
            wout[f] = (rounded(wo_ref[...]) * so_ref[...]).astype(BF)
        elif n == 1:
            g2 = column(g2_ref[pl.ds(f, 1), :])[:, 0:1]
            wup[own, :] = (rounded(wup_ref[...]) * g2).astype(BF)
        else:
            wdn[f] = (rounded(wdn_ref[...]) * sdn_ref[...]).astype(BF)
            xg[t] = x_ref[...]
            at = lax.broadcasted_iota(jnp.int32, (block, block), 0)
            low = at >= lax.broadcasted_iota(jnp.int32, (block, block), 1)
            grp_at = t * u_w // (gm_w // sw_ref.shape[0])
            mask[...] = jnp.where(low, sw_ref[grp_at], 0.0).astype(BF)
            bias[...] = column(sb_ref[pl.ds(grp_at, 1), :])

    steps = {
        "prep": prep, "z": z_hop, "fe": z_even, "fo": z_odd, "yd": y_done, "aga": ag_a, "agb": ag_b, "agc": ag_c,
        "age": ag_e, "agd": ag_d, "gating": gating, "stats": stats, "mixing": mixing, "a2s": a2_s, "a2w": a2_w,
        "outp": out_p, "ffup": ff_up, "rsa": rs_a, "rsb": rs_b, "rsc": rs_c, "rsd": rs_d,
    }
    for name, *rest in ORDER:
        steps[name](*rest)

    for s in streams.values():
        sent(s.whole, z_send.at[s.index], z_recv.at[s.index, 0, 0], to_up)
        if s.paired:
            sent(s.whole, y_send.at[s.index], y_recv.at[s.index], to_pair)
    for ph, buf in enumerate(gathered):
        for k in range(CHUNKS):
            rows = pl.ds(k * chunk, chunk)
            sent(buf.at[pl.ds(0, 3), rows, :], ag_send.at[ph, k], ag_recv.at[ph, k, 0], to_right)
            sent(buf.at[pl.ds(0, n_x), rows, :], agp_send.at[ph, k], agp_recv.at[ph, k], to_mate)
    for k in range(CHUNKS):
        sent(ps.at[k], rp_send.at[k], rp_recv.at[k, 0], to_mate)
        sent(qs.at[k, pl.ds(0, 3)], rr_send.at[k], rr_recv.at[k, 0], to_right)
        sent(st_x.at[pl.ds(0, 4), k], st_send.at[k], st_recv.at[k, 0], to_mate)
    sent(wmix.at[pl.ds(0, n_tp - 1)], a2_send.at[0], a2_recv.at[0], to_mate)


def per_device(dims, tokens, norm1_gain, weight_u, weight_v, scale_u, scale_v, mix_gain, spatial_weight,
               spatial_bias, weight_out, scale_out, norm2_gain, weight_up, scale_up, weight_down, scale_down):
    n_fs, n_tp = dims["fs"], dims["tp"]
    rows, width = tokens.shape
    feats = width * n_tp
    u_w, h_w = weight_u.shape[1], weight_up.shape[1]
    o_w, d_w = weight_out.shape[1], weight_down.shape[1]
    chunk = rows // CHUNKS
    block = spatial_weight.shape[1]
    n_x = n_tp // CORES
    if n_x != 4 or width != 2 * o_w or width != 2 * d_w:
        raise ValueError("unsupported mesh")
    args = (
        tokens, norm1_gain.reshape(n_fs, -1), weight_u, weight_v,
        scale_u.reshape(1, -1), scale_v.reshape(1, -1), mix_gain.reshape(1, -1), spatial_weight, spatial_bias,
        weight_out, scale_out.reshape(1, -1), norm2_gain.reshape(n_fs, -1), weight_up, scale_up.reshape(1, -1),
        weight_down, scale_down.reshape(1, -1),
    )
    dma = pltpu.SemaphoreType.DMA
    n_streams = 8
    scratch = [
        pltpu.VMEM((feats, 2 * u_w), BF),
        pltpu.VMEM((n_fs, u_w, o_w), BF),
        pltpu.VMEM((feats, h_w), BF),
        pltpu.VMEM((n_fs, h_w, d_w), BF),
        pltpu.VMEM((n_tp, rows, width), BF),
        pltpu.VMEM((n_tp, rows, width), BF),
        pltpu.VMEM((n_tp, rows, u_w), BF),
        pltpu.VMEM((n_tp, 2, u_w, o_w), BF),
        pltpu.VMEM((rows, u_w), F32),
        pltpu.VMEM((u_w, rows), F32),
        pltpu.VMEM((CHUNKS, 8, chunk), F32),
        pltpu.VMEM((CHUNKS, 8, chunk), F32),
        pltpu.VMEM((CHUNKS, 8, chunk), F32),
        pltpu.VMEM((4, CHUNKS, 8, chunk), F32),
        pltpu.VMEM((rows, h_w), BF),
        pltpu.VMEM((CHUNKS, n_x, chunk, width), BF),
        pltpu.VMEM((CHUNKS, n_x, chunk, width), BF),
        pltpu.VMEM((CHUNKS, n_x, chunk, width), BF),
        pltpu.VMEM((2, CHUNKS, chunk // 2, width), BF),
        pltpu.VMEM((2, CHUNKS, chunk, width), BF),
        pltpu.VMEM((block, block), BF),
        pltpu.VMEM((block, block), F32),
        dma((n_streams, 2, n_fs // 2)), dma((n_streams,)), dma((n_streams,)), dma((n_streams,)),
        dma((3, CHUNKS, 6)), dma((3, CHUNKS)), dma((3, CHUNKS)), dma((3, CHUNKS)),
        dma((CHUNKS, n_x)), dma((CHUNKS,)), dma((CHUNKS, 6)), dma((CHUNKS,)),
        dma((CHUNKS, 4)), dma((CHUNKS,)), dma((1,)), dma((1,)),
    ]
    vmem = pl.BlockSpec(memory_space=pltpu.VMEM)
    return pl.pallas_call(
        functools.partial(kernel, dims),
        out_shape=jax.ShapeDtypeStruct(tokens.shape, tokens.dtype),
        in_specs=[vmem] * len(args),
        out_specs=vmem,
        scratch_shapes=scratch,
        name="layer",
        compiler_params=pltpu.CompilerParams(
            collective_id=0, has_side_effects=True, vmem_limit_bytes=64 * 1000 * 1000),
    )(*args)


def solution(mesh):
    placed = (
        P(("grp", "fs"), "tp"), P(), P("fs", "tp"), P("fs", "tp"), P("tp"), P("tp"), P("tp"), P(), P(),
        P("tp", "fs"), P("fs"), P(), P("fs", "tp"), P("tp"), P("tp", "fs"), P("fs"),
    )
    return jax.shard_map(
        functools.partial(per_device, dict(mesh.shape)), mesh=mesh, in_specs=placed,
        out_specs=P(("grp", "fs"), "tp"), check_vma=False)
```

```python
import functools

import jax
import jax.numpy as jnp
from jax import lax
from jax.experimental import pallas as pl
from jax.experimental.pallas import tpu as pltpu
from jax.sharding import PartitionSpec as P

BF = jnp.bfloat16
F32 = jnp.float32
MESH = pl.DeviceIdType.MESH
EPS = 1e-06
CORES = 2
CHUNKS = 2
ROWS = 256
SWAP = {"uv": 64, "out": 64, "up": 48, "e": 16, "f": 16}
ORDER = (
    ("prep", 0), ("z", "outy", 1, 0), ("aga", 0, 1), ("z", "outy", 1, 1), ("fe", "uvy", 1, 0), ("prep", 1),
    ("z", "upy", 1, 0), ("fe", "uvy", 1, 1), ("prep", 2), ("z", "outy", 2, 1), ("z", "outy", 2, 0), ("aga", 0, 0),
    ("z", "upb", 1, 1), ("z", "ey", 1, 1), ("fo", "uvy", 2, 0), ("fe", "uvy", 2, 0), ("agb", 0, 1, 0),
    ("z", "outy", 3, 1), ("agb", 0, 1, 1), ("fo", "uvy", 2, 1), ("fe", "uvy", 2, 1), ("z", "upy", 2, 0),
    ("z", "upy", 1, 1), ("z", "outy", 4, 1), ("z", "outy", 3, 0), ("fe", "uvy", 3, 0), ("fe", "uvy", 3, 1),
    ("agb", 0, 0, 1), ("fo", "uvy", 3, 1), ("fo", "uvy", 3, 0), ("z", "upb", 1, 0), ("z", "outy", 4, 0),
    ("z", "ey", 1, 0), ("z", "outy", 5, 1), ("agc", 0, 1, 0), ("z", "eb", 1, 1), ("fo", "uvy", 4, 0),
    ("agb", 0, 0, 0), ("fe", "uvy", 4, 0), ("z", "ey", 2, 1), ("agc", 0, 0, 1), ("fo", "uvy", 4, 1),
    ("fe", "uvy", 4, 1), ("z", "outy", 5, 0), ("z", "outy", 6, 1), ("z", "upb", 2, 1), ("z", "upb", 2, 0),
    ("z", "eb", 1, 0), ("z", "fb", 1, 1), ("fo", "uvy", 5, 1), ("age", 0, 1, 1), ("fe", "uvy", 5, 0),
    ("agc", 0, 1, 1), ("fo", "uvy", 5, 0), ("age", 0, 1, 0), ("z", "outy", 7, 1), ("z", "outy", 6, 0),
    ("age", 0, 0, 0), ("z", "upy", 3, 0), ("z", "ey", 3, 1), ("z", "upy", 2, 1), ("agc", 0, 0, 0),
    ("z", "outy", 8, 1), ("z", "eb", 2, 1), ("agd", 0, 1), ("age", 0, 0, 1), ("z", "ey", 2, 0), ("z", "outy", 7, 0),
    ("z", "fb", 1, 0), ("z", "upb", 3, 1), ("z", "upb", 3, 0), ("yd", "uvy"), ("gating", 1), ("agd", 0, 0),
    ("gating", 0), ("z", "outy", 9, 1), ("z", "outy", 8, 0), ("z", "upy", 3, 1), ("z", "fb", 2, 1), ("z", "ey", 3, 0),
    ("z", "upy", 4, 0), ("z", "eb", 2, 0), ("mixing", 1), ("aga", 2, 1), ("z", "fy", 1, 0), ("z", "ey", 4, 0),
    ("z", "eb", 3, 1), ("mixing", 0), ("z", "upy", 4, 1), ("yd", "outy"), ("z", "ey", 4, 1), ("aga", 2, 0),
    ("z", "upy", 5, 0), ("agb", 2, 1, 0), ("z", "fy", 1, 1), ("a2s",), ("z", "eb", 4, 1), ("agb", 2, 1, 1),
    ("z", "upb", 4, 0), ("z", "eb", 3, 0), ("z", "ey", 5, 0), ("z", "upy", 5, 1), ("z", "upy", 6, 0),
    ("z", "fb", 3, 1), ("z", "ey", 5, 1), ("agc", 2, 1, 1), ("z", "upb", 4, 1), ("z", "eb", 4, 0), ("z", "ey", 6, 0),
    ("agc", 2, 1, 0), ("z", "fb", 2, 0), ("z", "upy", 6, 1), ("age", 2, 1, 0), ("agb", 2, 0, 1), ("agc", 2, 0, 1),
    ("z", "ey", 6, 1), ("age", 2, 1, 1), ("z", "upy", 7, 0), ("agb", 2, 0, 0), ("agd", 2, 1), ("z", "ey", 7, 0),
    ("z", "upb", 5, 1), ("age", 2, 0, 1), ("z", "fy", 2, 0), ("z", "upb", 5, 0), ("z", "upy", 7, 1),
    ("z", "ey", 7, 1), ("a2w",), ("outp", 1), ("agc", 2, 0, 0), ("z", "eb", 5, 1), ("aga", 1, 1), ("z", "upy", 8, 0),
    ("age", 2, 0, 0), ("z", "upb", 6, 1), ("z", "ey", 8, 0), ("fe", "uvy", 5, 1), ("z", "fy", 3, 0), ("agd", 2, 0),
    ("outp", 0), ("z", "fb", 4, 1), ("z", "fb", 3, 0), ("z", "upy", 8, 1), ("z", "eb", 5, 0), ("agb", 1, 1, 0),
    ("z", "upy", 9, 0), ("agb", 1, 1, 1), ("z", "ey", 8, 1), ("aga", 1, 0), ("z", "fy", 2, 1), ("z", "eb", 6, 1),
    ("z", "ey", 9, 0), ("z", "fy", 4, 0), ("z", "upb", 6, 0), ("z", "upb", 7, 1), ("z", "fb", 4, 0), ("agc", 1, 1, 0),
    ("z", "fy", 3, 1), ("z", "eb", 7, 1), ("z", "fb", 5, 1), ("agc", 1, 1, 1), ("z", "fy", 5, 0), ("z", "eb", 6, 0),
    ("age", 1, 1, 0), ("z", "fy", 4, 1), ("z", "upb", 7, 0), ("age", 1, 1, 1), ("z", "upb", 8, 1), ("z", "fy", 6, 0),
    ("agb", 1, 0, 0), ("agb", 1, 0, 1), ("z", "eb", 8, 1), ("z", "eb", 7, 0), ("z", "fb", 5, 0), ("z", "upb", 8, 0),
    ("agd", 1, 1), ("agc", 1, 0, 1), ("z", "fy", 5, 1), ("z", "fb", 6, 1), ("z", "upb", 9, 1), ("agc", 1, 0, 0),
    ("z", "fy", 7, 0), ("yd", "upy"), ("ffup", 1), ("z", "eb", 9, 1), ("age", 1, 0, 1), ("yd", "ey"),
    ("z", "eb", 8, 0), ("z", "fy", 6, 1), ("rsa", 1, 0), ("age", 1, 0, 0), ("z", "fb", 6, 0), ("rsa", 1, 1),
    ("z", "fb", 7, 1), ("rsb", 1, 0), ("z", "fy", 8, 0), ("agd", 1, 0), ("rsb", 1, 1), ("z", "fy", 7, 1), ("ffup", 0),
    ("z", "fy", 9, 0), ("z", "fb", 8, 1), ("z", "fb", 7, 0), ("rsc", 1, 1), ("rsc", 1, 0), ("z", "fy", 8, 1),
    ("rsa", 0, 0), ("rsa", 0, 1), ("rsb", 0, 0), ("rsb", 0, 1), ("yd", "fy"), ("z", "fb", 9, 1), ("z", "fb", 8, 0),
    ("rsa", 2, 0), ("rsd", 1), ("rsb", 2, 0), ("rsa", 3, 0), ("rsc", 0, 0), ("rsc", 0, 1), ("rsa", 2, 1),
    ("rsb", 3, 0), ("rsb", 2, 1), ("rsc", 2, 0), ("rsa", 3, 1), ("rsc", 2, 1), ("rsb", 3, 1), ("rsd", 0),
    ("rsc", 3, 1), ("rsc", 3, 0), ("rsd", 2), ("rsd", 3),
)


class Stream:
    def __init__(self, name, ref, rows, whole, paired):
        self.name, self.ref, self.rows, self.whole, self.paired = name, ref, rows, whole, paired


def kernel(
    dims,
    x_ref, g1_ref, wu_ref, wv_ref, su_ref, sv_ref, mg_ref, sw_ref, sb_ref, wo_ref, so_ref,
    g2_ref, wup_ref, sup_ref, wdn_ref, sdn_ref,
    out_ref,
    wuv, wout, wup, wdn, xg, rg, gg, wmix, ub, vt, st, hid,
    ps, pr, qs, op, fi, mask, bias, total_e,
    z_recv, z_send, y_recv, y_send, ag_recv, ag_send, agp_recv, agp_send,
    rp_recv, rp_send, rr_recv, rr_send, st_recv, st_send, a2_recv, a2_send,
):
    n_fs, n_tp = dims["fs"], dims["tp"]
    n_x = n_tp // CORES
    half_ring = n_fs // 2
    total_rows, width = x_ref.shape
    feats = width * n_tp
    u_w = wu_ref.shape[1]
    k_fs = wu_ref.shape[0]
    h_w = wup_ref.shape[1]
    gm_w = u_w * n_tp
    chunk = total_rows // CHUNKS
    half = chunk // 2
    block = sw_ref.shape[1]
    pair = dims["grp"] % 2 == 0

    g = lax.axis_index("grp")
    f = lax.axis_index("fs")
    t = lax.axis_index("tp")
    cx = t // CORES
    core = t % CORES
    par = g % 2

    def chip(d):
        return (cx + d) % n_x

    def tp_of(d):
        return chip(d) * CORES + core

    to_right, to_left, to_opp = {"tp": tp_of(1)}, {"tp": tp_of(n_x - 1)}, {"tp": tp_of(2)}
    to_mate = {"tp": cx * CORES + 1 - core}
    to_up, to_down = {"fs": (f + 1) % n_fs}, {"fs": (f + n_fs - 1) % n_fs}
    to_pair = {"grp": g + 1 - 2 * par}

    to_up2, to_down2 = {"fs": (f + 2) % n_fs}, {"fs": (f + n_fs - 2) % n_fs}
    others = [{"tp": chip(rel) * CORES + (core + c) % CORES} for rel in range(n_x) for c in range(CORES) if rel or c]
    neighbours = others + [to_up, to_down, to_up2, to_down2]
    if pair:
        neighbours.append(to_pair)
    barrier = pltpu.get_barrier_semaphore()
    for n in neighbours:
        pl.semaphore_signal(barrier, inc=1, device_id=n, device_id_type=MESH)
    pl.semaphore_wait(barrier, len(neighbours))

    def rcopy(src, dst, ss, rs, dev):
        return pltpu.make_async_remote_copy(
            src_ref=src, dst_ref=dst, send_sem=ss, recv_sem=rs, device_id=dev, device_id_type=MESH)

    def got(ref, sem, spare, dev):
        rcopy(ref, ref, spare, sem, dev).wait_recv()

    def sent(ref, sem, spare, dev):
        rcopy(ref, ref, sem, spare, dev).wait_send()

    def rows_2d(ref, start):
        def at(slot, rows):
            return ref.at[pl.ds(pl.multiple_of(slot * k_fs + start, 16), rows), :]
        return at

    def rows_3d(ref, start):
        def at(slot, rows):
            return ref.at[slot, pl.ds(pl.multiple_of(start, 16), rows), :]
        return at

    def whole_2d(ref, rows):
        return ref.at[pl.ds(0, (n_fs - 1) * rows), :]

    def whole_3d(ref, rows):
        return ref.at[pl.ds(0, n_fs - 1), pl.ds(0, rows), :]

    def make(name, ref, three, first, own_rows, swap):
        def at(r, start):
            return (rows_3d if three else rows_2d)(r, first + start)

        whole = whole_3d if three else whole_2d
        result = []
        if pair and swap:
            shared = own_rows - 2 * swap
            result.append(Stream(name + "y", at(ref, par * (own_rows - swap)), swap, whole(ref, swap), True))
            if shared:
                result.append(Stream(name + "b", at(ref, swap), shared, whole(ref, shared), False))
        else:
            result.append(Stream(name + "y", at(ref, 0), own_rows, whole(ref, own_rows), False))
        return result

    streams = {}
    dn_half = k_fs // 2
    for s in (make("uv", wuv, False, 0, k_fs, SWAP["uv"]) + make("out", wout, True, 0, u_w, SWAP["out"])
              + make("up", wup, False, 0, k_fs, SWAP["up"]) + make("e", wdn, False, 0, dn_half, SWAP["e"])
              + make("f", wdn, False, dn_half, dn_half, SWAP["f"])):
        s.index = len(streams)
        streams[s.name] = s

    def z_dirs(s, hop):
        return (0, 1) if hop < half_ring else (s.index % 2,)

    def piece_at(s, d, back):
        return s.ref((f + (n_fs - back if d == 0 else back)) % n_fs, s.rows)

    def z_got(s, d, hop):
        piece = piece_at(s, d, hop)
        got(piece, z_recv.at[s.index, d, hop - 1], z_send.at[s.index], to_up)
        return piece

    def z_send_on(s, d, back, hop, to):
        piece = piece_at(s, d, back)
        rcopy(piece, piece, z_send.at[s.index], z_recv.at[s.index, d, hop - 1], to).start()

    def to_partner(s, piece):
        if s.paired:
            rcopy(piece, piece, y_send.at[s.index], y_recv.at[s.index], to_pair).start()

    def z_hop(name, hop, d):
        s = streams[name]
        if hop > 1 and d in z_dirs(s, hop - 1):
            to_partner(s, z_got(s, d, hop - 1))
        if hop <= half_ring and d in z_dirs(s, hop):
            z_send_on(s, d, hop - 1, hop, to_down if d else to_up)

    def z_even(name, stage, d):
        s = streams[name]
        even = 2 * (stage - 1)
        arrived = stage > 1 and d in z_dirs(s, even)
        if arrived:
            piece = z_got(s, d, even)
        if even < half_ring:
            for step, to in ((2, to_down2 if d else to_up2), (1, to_down if d else to_up)):
                if d in z_dirs(s, even + step):
                    z_send_on(s, d, even, even + step, to)
        if arrived:
            to_partner(s, piece)

    def z_odd(name, stage, d):
        s = streams[name]
        to_partner(s, z_got(s, d, 2 * stage - 3))

    def y_done(name):
        s = streams[name]
        if not s.paired:
            return
        got(s.whole, y_recv.at[s.index], y_send.at[s.index], to_pair)

    def ag_rows(buf, slot, start, rows):
        return buf.at[slot, pl.ds(start, rows), :]

    gathered = (xg, rg, gg)

    def to_other_core(ph, k, piece):
        rcopy(piece, piece, agp_send.at[ph, k], agp_recv.at[ph, k], to_mate).start()

    def ag_a(ph, k):
        buf = gathered[ph]

        def src(at, n):
            return x_ref.at[pl.ds(at, n), :] if ph == 0 else ag_rows(buf, t, at, n)

        for n, to, lo in ((0, to_right, 0), (1, to_right, half), (2, to_left, half), (3, to_left, 0)):
            at = k * chunk + lo
            rcopy(src(at, half), ag_rows(buf, t, at, half), ag_send.at[ph, k], ag_recv.at[ph, k, n], to).start()
        at = k * chunk
        rcopy(src(at, chunk), ag_rows(buf, t, at, chunk), agp_send.at[ph, k], agp_recv.at[ph, k], to_mate).start()

    SIDES = ((n_x - 1, 0, to_right), (1, half, to_left))

    def ag_b(ph, k, side):
        chip_at, lo, to = SIDES[side]
        part = ag_rows(gathered[ph], tp_of(chip_at), k * chunk + lo, half)
        got(part, ag_recv.at[ph, k, 2 * side], ag_send.at[ph, k], to)
        rcopy(part, part, ag_send.at[ph, k], ag_recv.at[ph, k, 4 + side], to).start()

    def ag_c(ph, k, side):
        chip_at, lo, to = SIDES[side]
        part = ag_rows(gathered[ph], tp_of(chip_at), k * chunk + half - lo, half)
        got(part, ag_recv.at[ph, k, 2 * side + 1], ag_send.at[ph, k], to)
        to_other_core(ph, k, ag_rows(gathered[ph], tp_of(chip_at), k * chunk, chunk))

    def ag_e(ph, k, side):
        part = ag_rows(gathered[ph], tp_of(2), k * chunk + SIDES[side][1], half)
        got(part, ag_recv.at[ph, k, 4 + side], ag_send.at[ph, k], to_right)
        to_other_core(ph, k, part)

    def ag_d(ph, k):
        got(gathered[ph].at[pl.ds(0, n_x), pl.ds(k * chunk, chunk), :], agp_recv.at[ph, k], agp_send.at[ph, k], to_mate)

    def a2_s():
        for n, to in enumerate(others):
            rcopy(wout.at[pl.ds(2 * to["tp"], 2)], wmix.at[t], a2_send.at[0], a2_recv.at[0], to).start()
        wmix[t] = wout[pl.ds(2 * t, 2)]

    def a2_w():
        got(wmix.at[pl.ds(0, n_tp - 1)], a2_recv.at[0], a2_send.at[0], to_mate)

    def out_p(k):
        rows = pl.ds(k * chunk, chunk)
        left = jnp.concatenate([gg[j, rows, :] for j in range(n_tp)], axis=1)
        right = jnp.concatenate(
            [jnp.concatenate([wmix[j, 0], wmix[j, 1]], axis=1) for j in range(n_tp)], axis=0)
        total = jnp.dot(left, right, preferred_element_type=F32)
        rg[t, rows, :] = (x_ref[rows, :].astype(F32) + total).astype(BF)

    PAIRS = ((2, 1), (3, 0))

    def product(u, rels, c):
        k, e = u % CHUNKS, u // CHUNKS
        parts = []
        for rel in rels:
            j = chip(rel) * CORES + c
            for shard in (2 * j, 2 * j + 1):
                at = pl.multiple_of(shard * k_fs + e * dn_half, dn_half)
                parts.append(wdn[pl.ds(at, dn_half), :])
        both = lax.dot_general(hid[pl.ds(k * chunk, chunk), :], jnp.concatenate(parts, axis=0),
                               (((1,), (1,)), ((), ())), preferred_element_type=F32)
        return (rels[0], both[:, :k_fs]), (rels[1], both[:, k_fs:])

    def rs_a(k, p):
        for rel, value in product(k, PAIRS[p], 1 - core):
            ps[k, rel] = value.astype(BF)
            rcopy(ps.at[k, rel], pr.at[k, rel], rp_send.at[k], rp_recv.at[k, rel], to_mate).start()

    def rs_b(k, p):
        ss = rr_send.at[k]
        for rel, value in product(k, PAIRS[p], core):
            got(pr.at[k, rel], rp_recv.at[k, rel], rp_send.at[k], to_mate)
            qs[k, rel] = (value + pr[k, rel].astype(F32)).astype(BF)
            low, high = qs.at[k, rel, pl.ds(0, half), :], qs.at[k, rel, pl.ds(half, half), :]
            if rel == 2:
                rcopy(low, op.at[0, k], ss, rr_recv.at[k, 0], to_right).start()
                rcopy(high, op.at[1, k], ss, rr_recv.at[k, 1], to_left).start()
            elif rel == 1:
                rcopy(high, fi.at[0, k, pl.ds(half, half), :], ss, rr_recv.at[k, 2], to_right).start()
            elif rel == 3:
                rcopy(low, fi.at[1, k, pl.ds(0, half), :], ss, rr_recv.at[k, 3], to_left).start()

    def rs_c(k, side):
        ss = rr_send.at[k]
        rel, (_, lo, to) = (1, 3)[side], SIDES[side]
        got(op.at[side, k], rr_recv.at[k, side], ss, to)
        rows = pl.ds(lo, half)
        qs[k, rel, rows, :] = (qs[k, rel, rows, :].astype(F32) + op[side, k].astype(F32)).astype(BF)
        rcopy(qs.at[k, rel, rows, :], fi.at[side, k, rows, :], ss, rr_recv.at[k, 4 + side], to).start()

    def rs_d(k):
        ss = rr_send.at[k]
        for n, side, lo in ((2, 0, half), (3, 1, 0), (4, 0, 0), (5, 1, half)):
            got(fi.at[side, k, pl.ds(lo, half), :], rr_recv.at[k, n], ss, to_right)
        for r in range(0, chunk, ROWS):
            rows, at = pl.ds(r, ROWS), pl.ds((k % CHUNKS) * chunk + r, ROWS)
            total = qs[k, 0, rows, :].astype(F32) + fi[0, k, rows, :].astype(F32) + fi[1, k, rows, :].astype(F32)
            if k < CHUNKS:
                total_e[at, :] = total
            else:
                first, h = total_e[at, :], dn_half
                total = jnp.concatenate([first[:, :h], total[:, :h], first[:, h:], total[:, h:]], axis=1)
                out_ref[at, :] = (rg[t, at, :].astype(F32) + total).astype(BF)

    def column(row):
        return jnp.broadcast_to(row, (row.shape[1], row.shape[1])).T

    def joined(buf, r):
        parts = [buf[j, pl.ds(r, ROWS), :] for j in range(n_tp)]
        squares = None
        for part in parts:
            wide = part.astype(F32)
            squares = wide * wide if squares is None else squares + wide * wide
        inv = lax.rsqrt(jnp.sum(squares, axis=1, keepdims=True) / feats + EPS)
        return jnp.concatenate(parts, axis=1), inv

    def gating(k):
        scale_uv = jnp.concatenate([su_ref[...], sv_ref[...]], axis=1)
        for r in range(0, chunk, ROWS):
            at = k * chunk + r
            lhs, inv = joined(xg, at)
            pre = jnp.dot(lhs, wuv[...], preferred_element_type=F32) * inv * scale_uv
            act = jax.nn.gelu(pre)
            ub[pl.ds(at, ROWS), :] = act[:, :u_w]
            turned = act[:, u_w:].T
            vt[:, pl.ds(at, ROWS)] = turned
            for sums, first in ((jnp.sum(turned, axis=0, keepdims=True), 0),
                                (jnp.sum(turned * turned, axis=0, keepdims=True), chunk // block)):
                for b in range(0, ROWS, block):
                    st[t, k, pl.ds(first + (r + b) // block, 1), :] = sums[:, b:b + block]
        for to in others:
            rcopy(st.at[t, k], st.at[t, k], st_send.at[k], st_recv.at[k], to).start()

    def mixing(k):
        got(st.at[pl.ds(0, n_tp - 1), k], st_recv.at[k], st_send.at[k], to_mate)
        total = st[0, k]
        for n in range(1, n_tp):
            total = total + st[n, k]
        blocks = chunk // block
        mean = total[:blocks] / gm_w
        square = total[blocks:2 * blocks] / gm_w
        scale = lax.rsqrt(square - mean * mean + EPS)
        gain = column(mg_ref[...])[:, 0:1]
        for b in range(0, chunk, block):
            at = k * chunk + b
            n = b // block
            v_norm = ((vt[:, pl.ds(at, block)] - mean[n:n + 1]) * scale[n:n + 1] * gain).astype(BF)
            mixed = lax.dot_general(mask[...], v_norm, (((1,), (1,)), ((), ())), preferred_element_type=F32)
            gg[t, pl.ds(at, block), :] = (ub[pl.ds(at, block), :] * (mixed + bias[...])).astype(BF)

    def ff_up(k):
        for r in range(0, chunk, ROWS):
            at = k * chunk + r
            lhs, inv = joined(rg, at)
            for n in range(0, h_w, 256):
                cols = pl.ds(n, 256)
                acc = jnp.dot(lhs, wup[:, n:n + 256], preferred_element_type=F32)
                acc = jnp.maximum(acc * inv * sup_ref[:, n:n + 256], 0.0)
                hid[pl.ds(at, ROWS), cols] = (acc * acc).astype(BF)

    def rounded(w):
        return w.astype(BF).astype(F32)

    own = pl.ds(pl.multiple_of(f * k_fs, k_fs), k_fs)

    def prep(n):
        if n == 0:
            g1 = column(g1_ref[pl.ds(f, 1), :])
            wuv[own, :] = (jnp.concatenate([rounded(wu_ref[...]) * g1, rounded(wv_ref[...]) * g1], axis=1)).astype(BF)
            wout[f] = (rounded(wo_ref[...]) * so_ref[...]).astype(BF)
        elif n == 1:
            g2 = column(g2_ref[pl.ds(f, 1), :])[:, 0:1]
            wup[own, :] = (rounded(wup_ref[...]) * g2).astype(BF)
        else:
            wdn[own, :] = (rounded(wdn_ref[...]) * sdn_ref[...]).T.astype(BF)
            xg[t] = x_ref[...]
            at = lax.broadcasted_iota(jnp.int32, (block, block), 0)
            low = at >= lax.broadcasted_iota(jnp.int32, (block, block), 1)
            grp_at = t * u_w // (gm_w // sw_ref.shape[0])
            mask[...] = jnp.where(low, sw_ref[grp_at], 0.0).astype(BF)
            bias[...] = column(sb_ref[pl.ds(grp_at, 1), :])

    steps = {
        "prep": prep, "z": z_hop, "fe": z_even, "fo": z_odd, "yd": y_done, "aga": ag_a, "agb": ag_b, "agc": ag_c,
        "age": ag_e, "agd": ag_d, "gating": gating, "mixing": mixing, "a2s": a2_s, "a2w": a2_w,
        "outp": out_p, "ffup": ff_up, "rsa": rs_a, "rsb": rs_b, "rsc": rs_c, "rsd": rs_d,
    }
    for name, *rest in ORDER:
        steps[name](*rest)

    for s in streams.values():
        sent(s.whole, z_send.at[s.index], z_recv.at[s.index, 0, 0], to_up)
        if s.paired:
            sent(s.whole, y_send.at[s.index], y_recv.at[s.index], to_pair)
    for ph, buf in enumerate(gathered):
        for k in range(CHUNKS):
            rows = pl.ds(k * chunk, chunk)
            sent(buf.at[pl.ds(0, 3), rows, :], ag_send.at[ph, k], ag_recv.at[ph, k, 0], to_right)
            sent(buf.at[pl.ds(0, n_x), rows, :], agp_send.at[ph, k], agp_recv.at[ph, k], to_mate)
    for u in range(2 * CHUNKS):
        sent(ps.at[u], rp_send.at[u], rp_recv.at[u, 0], to_mate)
        sent(qs.at[u, pl.ds(0, 3)], rr_send.at[u], rr_recv.at[u, 0], to_right)
    for k in range(CHUNKS):
        sent(st.at[pl.ds(0, n_tp - 1), k], st_send.at[k], st_recv.at[k], to_mate)
    sent(wmix.at[pl.ds(0, n_tp - 1)], a2_send.at[0], a2_recv.at[0], to_mate)


def per_device(dims, tokens, norm1_gain, weight_u, weight_v, scale_u, scale_v, mix_gain, spatial_weight,
               spatial_bias, weight_out, scale_out, norm2_gain, weight_up, scale_up, weight_down, scale_down):
    n_fs, n_tp = dims["fs"], dims["tp"]
    rows, width = tokens.shape
    feats = width * n_tp
    u_w, h_w = weight_u.shape[1], weight_up.shape[1]
    o_w, d_w = weight_out.shape[1], weight_down.shape[1]
    chunk = rows // CHUNKS
    block = spatial_weight.shape[1]
    n_x = n_tp // CORES
    if n_x != 4 or width != 2 * o_w or width != 2 * d_w:
        raise ValueError("unsupported mesh")
    args = (
        tokens, norm1_gain.reshape(n_fs, -1), weight_u, weight_v,
        scale_u.reshape(1, -1), scale_v.reshape(1, -1), mix_gain.reshape(1, -1), spatial_weight, spatial_bias,
        weight_out, scale_out.reshape(1, -1), norm2_gain.reshape(n_fs, -1), weight_up, scale_up.reshape(1, -1),
        weight_down, scale_down.reshape(1, -1),
    )
    dma = pltpu.SemaphoreType.DMA
    n_streams = 8
    scratch = [
        pltpu.VMEM((feats, 2 * u_w), BF),
        pltpu.VMEM((n_fs, u_w, o_w), BF),
        pltpu.VMEM((feats, h_w), BF),
        pltpu.VMEM((feats, h_w), BF),
        pltpu.VMEM((n_tp, rows, width), BF),
        pltpu.VMEM((n_tp, rows, width), BF),
        pltpu.VMEM((n_tp, rows, u_w), BF),
        pltpu.VMEM((n_tp, 2, u_w, o_w), BF),
        pltpu.VMEM((rows, u_w), F32),
        pltpu.VMEM((u_w, rows), F32),
        pltpu.VMEM((n_tp, CHUNKS, 2 * chunk // block, block), F32),
        pltpu.VMEM((rows, h_w), BF),
        pltpu.VMEM((2 * CHUNKS, n_x, chunk, d_w), BF),
        pltpu.VMEM((2 * CHUNKS, n_x, chunk, d_w), BF),
        pltpu.VMEM((2 * CHUNKS, n_x, chunk, d_w), BF),
        pltpu.VMEM((2, 2 * CHUNKS, chunk // 2, d_w), BF),
        pltpu.VMEM((2, 2 * CHUNKS, chunk, d_w), BF),
        pltpu.VMEM((block, block), BF),
        pltpu.VMEM((block, block), F32),
        pltpu.VMEM((rows, d_w), F32),
        dma((n_streams, 2, n_fs // 2)), dma((n_streams,)), dma((n_streams,)), dma((n_streams,)),
        dma((3, CHUNKS, 6)), dma((3, CHUNKS)), dma((3, CHUNKS)), dma((3, CHUNKS)),
        dma((2 * CHUNKS, n_x)), dma((2 * CHUNKS,)), dma((2 * CHUNKS, 6)), dma((2 * CHUNKS,)),
        dma((CHUNKS,)), dma((CHUNKS,)), dma((1,)), dma((1,)),
    ]
    vmem = pl.BlockSpec(memory_space=pltpu.VMEM)
    return pl.pallas_call(
        functools.partial(kernel, dims),
        out_shape=jax.ShapeDtypeStruct(tokens.shape, tokens.dtype),
        in_specs=[vmem] * len(args),
        out_specs=vmem,
        scratch_shapes=scratch,
        name="layer",
        compiler_params=pltpu.CompilerParams(
            collective_id=0, has_side_effects=True, vmem_limit_bytes=64 * 1000 * 1000),
    )(*args)


def solution(mesh):
    placed = (
        P(("grp", "fs"), "tp"), P(), P("fs", "tp"), P("fs", "tp"), P("tp"), P("tp"), P("tp"), P(), P(),
        P("tp", "fs"), P("fs"), P(), P("fs", "tp"), P("tp"), P("tp", "fs"), P("fs"),
    )
    return jax.shard_map(
        functools.partial(per_device, dict(mesh.shape)), mesh=mesh, in_specs=placed,
        out_specs=P(("grp", "fs"), "tp"), check_vma=False)
```

```python
import functools

import jax
import jax.numpy as jnp
from jax import lax
from jax.experimental import pallas as pl
from jax.experimental.pallas import tpu as pltpu
from jax.sharding import PartitionSpec as P

BF = jnp.bfloat16
F32 = jnp.float32
MESH = pl.DeviceIdType.MESH
EPS = 1e-06
CORES = 2
CHUNKS = 2
ROWS = 256
INPUTS = 16
SWAP = {"uv": 64, "out": 64, "up": 48, "e": 16, "f": 16}
ORDER = (
    ("prep", 0), ("z", "outy", 1, 0), ("fe", "uvy", 1, 0), ("aga", 0, 0), ("z", "outy", 1, 1), ("fe", "uvy", 1, 1),
    ("prep", 1), ("z", "upy", 1, 0), ("z", "outy", 2, 0), ("z", "upb", 1, 1), ("prep", 2), ("z", "ey", 1, 1),
    ("z", "outy", 2, 1), ("fo", "uvy", 2, 0), ("fe", "uvy", 2, 0), ("aga", 0, 1), ("fo", "uvy", 2, 1),
    ("fe", "uvy", 2, 1), ("z", "upy", 2, 0), ("z", "outy", 3, 0), ("z", "eb", 1, 1), ("agb", 0, 0, 0),
    ("z", "outy", 3, 1), ("z", "ey", 2, 1), ("fe", "uvy", 3, 0), ("fe", "uvy", 3, 1), ("agb", 0, 1, 1),
    ("z", "ey", 1, 0), ("agb", 0, 0, 1), ("fo", "uvy", 3, 0), ("z", "outy", 4, 0), ("z", "fb", 1, 0),
    ("fo", "uvy", 3, 1), ("z", "outy", 4, 1), ("z", "fy", 1, 1), ("agc", 0, 0, 0), ("z", "eb", 2, 1),
    ("fo", "uvy", 4, 1), ("fe", "uvy", 4, 0), ("fe", "uvy", 4, 1), ("agb", 0, 1, 0), ("z", "outy", 5, 1),
    ("z", "outy", 5, 0), ("z", "upy", 1, 1), ("z", "upb", 1, 0), ("fo", "uvy", 4, 0), ("z", "fb", 1, 1),
    ("z", "eb", 1, 0), ("age", 0, 1, 1), ("fo", "uvy", 5, 1), ("fo", "uvy", 5, 0), ("age", 0, 0, 0),
    ("fe", "uvy", 5, 0), ("z", "outy", 6, 1), ("agc", 0, 1, 1), ("agc", 0, 1, 0), ("z", "ey", 3, 1),
    ("z", "outy", 6, 0), ("z", "ey", 2, 0), ("z", "upy", 3, 0), ("age", 0, 0, 1), ("z", "upy", 2, 1),
    ("agc", 0, 0, 1), ("z", "outy", 7, 1), ("z", "upb", 2, 1), ("z", "outy", 7, 0), ("z", "eb", 2, 0),
    ("age", 0, 1, 0), ("yd", "uvy"), ("agd", 0, 0), ("gating", 0), ("agd", 0, 1), ("z", "ey", 3, 0),
    ("z", "eb", 3, 1), ("gating", 1), ("z", "outy", 8, 1), ("z", "upy", 3, 1), ("z", "upy", 4, 0), ("z", "upb", 2, 0),
    ("z", "outy", 8, 0), ("z", "upb", 3, 1), ("mixing", 0), ("z", "outy", 9, 1), ("z", "fb", 2, 1),
    ("fe", "uvy", 5, 1), ("aga", 2, 0), ("z", "eb", 3, 0), ("mixing", 1), ("z", "upy", 5, 0), ("z", "ey", 4, 0),
    ("z", "upy", 4, 1), ("aga", 2, 1), ("agb", 2, 0, 1), ("agb", 2, 0, 0), ("z", "eb", 4, 0), ("z", "upb", 3, 0),
    ("z", "fy", 2, 1), ("z", "eb", 4, 1), ("z", "ey", 4, 1), ("z", "upy", 6, 0), ("z", "upy", 5, 1),
    ("z", "upb", 4, 1), ("agb", 2, 1, 1), ("yd", "outy"), ("a2s",), ("agb", 2, 1, 0), ("z", "eb", 5, 1),
    ("agc", 2, 0, 0), ("z", "ey", 5, 0), ("age", 2, 0, 1), ("z", "fy", 1, 0), ("z", "fb", 2, 0), ("z", "upy", 7, 0),
    ("z", "ey", 5, 1), ("agc", 2, 0, 1), ("z", "upy", 6, 1), ("z", "ey", 6, 0), ("age", 2, 0, 0), ("z", "upb", 4, 0),
    ("z", "upb", 5, 1), ("age", 2, 1, 1), ("z", "fy", 2, 0), ("z", "fb", 3, 1), ("z", "upy", 8, 0), ("z", "ey", 7, 0),
    ("z", "upy", 7, 1), ("z", "ey", 6, 1), ("a2w",), ("agd", 2, 0), ("outp", 0), ("aga", 1, 0), ("z", "upb", 6, 1),
    ("z", "upb", 5, 0), ("agc", 2, 1, 0), ("agc", 2, 1, 1), ("age", 2, 1, 0), ("z", "eb", 6, 1), ("z", "eb", 5, 0),
    ("agd", 2, 1), ("outp", 1), ("z", "upy", 9, 0), ("z", "upy", 8, 1), ("z", "ey", 8, 0), ("z", "ey", 7, 1),
    ("z", "fy", 3, 0), ("z", "fb", 3, 0), ("z", "fb", 4, 1), ("agb", 1, 0, 0), ("z", "upb", 7, 1), ("z", "upb", 6, 0),
    ("agb", 1, 0, 1), ("z", "ey", 9, 0), ("z", "ey", 8, 1), ("z", "fy", 4, 0), ("z", "fy", 3, 1), ("z", "eb", 6, 0),
    ("z", "eb", 7, 1), ("aga", 1, 1), ("agc", 1, 0, 1), ("z", "fb", 4, 0), ("z", "fb", 5, 1), ("agc", 1, 0, 0),
    ("z", "fy", 5, 0), ("z", "fy", 4, 1), ("age", 1, 0, 1), ("z", "upb", 8, 1), ("age", 1, 0, 0), ("z", "upb", 7, 0),
    ("z", "eb", 8, 1), ("agb", 1, 1, 1), ("agb", 1, 1, 0), ("z", "eb", 7, 0), ("z", "fy", 6, 0), ("agd", 1, 0),
    ("z", "fy", 5, 1), ("z", "fb", 6, 1), ("yd", "upy"), ("z", "upb", 9, 1), ("z", "fb", 5, 0), ("z", "upb", 8, 0),
    ("ffup", 0), ("z", "fy", 6, 1), ("z", "fy", 7, 0), ("agc", 1, 1, 0), ("z", "eb", 9, 1), ("z", "eb", 8, 0),
    ("yd", "ey"), ("agc", 1, 1, 1), ("age", 1, 1, 1), ("rsa", 0, 0), ("z", "fb", 6, 0), ("age", 1, 1, 0),
    ("z", "fb", 7, 1), ("rsa", 0, 1), ("rsb", 0, 0), ("agd", 1, 1), ("z", "fy", 7, 1), ("z", "fy", 8, 0),
    ("rsb", 0, 1), ("ffup", 1), ("z", "fb", 8, 1), ("z", "fb", 7, 0), ("z", "fy", 9, 0), ("z", "fy", 8, 1),
    ("rsc", 0, 1), ("rsc", 0, 0), ("rsa", 1, 0), ("rsa", 1, 1), ("rsb", 1, 0), ("rsb", 1, 1), ("z", "fb", 9, 1),
    ("z", "fb", 8, 0), ("yd", "fy"), ("rsa", 2, 0), ("rsd", 0), ("rsb", 2, 0), ("rsa", 3, 1), ("rsc", 1, 1),
    ("rsa", 3, 0), ("rsb", 3, 1), ("rsc", 1, 0), ("rsb", 3, 0), ("rsa", 2, 1), ("rsb", 2, 1), ("rsc", 2, 0),
    ("rsc", 2, 1), ("rsd", 1), ("rsc", 3, 0), ("rsc", 3, 1), ("rsd", 2), ("rsd", 3),
)


class Stream:
    def __init__(self, name, ref, rows, whole, paired):
        self.name, self.ref, self.rows, self.whole, self.paired = name, ref, rows, whole, paired


def kernel(
    dims,
    *refs,
):
    given, out_ref, held, (
        wuv, wout, wup, wdn, xg, rg, gg, wmix, ub, vt, st, hid,
        ps, pr, qs, op, fi, mask, bias, total_e,
        z_recv, z_send, y_recv, y_send, ag_recv, ag_send, agp_recv, agp_send,
        rp_recv, rp_send, rr_recv, rr_send, st_recv, st_send, a2_recv, a2_send, in_sem,
    ) = refs[:INPUTS], refs[INPUTS], refs[INPUTS + 1:2 * INPUTS + 1], refs[2 * INPUTS + 1:]
    (
        x_ref, g1_ref, wu_ref, wv_ref, su_ref, sv_ref, mg_ref, sw_ref, sb_ref, wo_ref, so_ref,
        g2_ref, wup_ref, sup_ref, wdn_ref, sdn_ref,
    ) = held
    n_fs, n_tp = dims["fs"], dims["tp"]
    n_x = n_tp // CORES
    half_ring = n_fs // 2
    total_rows, width = x_ref.shape
    feats = width * n_tp
    u_w = wu_ref.shape[1]
    k_fs = wu_ref.shape[0]
    h_w = wup_ref.shape[1]
    gm_w = u_w * n_tp
    chunk = total_rows // CHUNKS
    half = chunk // 2
    block = sw_ref.shape[1]
    pair = dims["grp"] % 2 == 0

    g = lax.axis_index("grp")
    f = lax.axis_index("fs")
    t = lax.axis_index("tp")
    cx = t // CORES
    core = t % CORES
    par = g % 2

    def chip(d):
        return (cx + d) % n_x

    def tp_of(d):
        return chip(d) * CORES + core

    to_right, to_left, to_opp = {"tp": tp_of(1)}, {"tp": tp_of(n_x - 1)}, {"tp": tp_of(2)}
    to_mate = {"tp": cx * CORES + 1 - core}
    to_up, to_down = {"fs": (f + 1) % n_fs}, {"fs": (f + n_fs - 1) % n_fs}
    to_pair = {"grp": g + 1 - 2 * par}

    to_up2, to_down2 = {"fs": (f + 2) % n_fs}, {"fs": (f + n_fs - 2) % n_fs}
    others = [{"tp": chip(rel) * CORES + (core + c) % CORES} for rel in range(n_x) for c in range(CORES) if rel or c]
    neighbours = others + [to_up, to_down, to_up2, to_down2]
    if pair:
        neighbours.append(to_pair)
    barrier = pltpu.get_barrier_semaphore()
    for n in neighbours:
        pl.semaphore_signal(barrier, inc=1, device_id=n, device_id_type=MESH)
    loads = [pltpu.make_async_copy(a, b, in_sem.at[n]) for n, (a, b) in enumerate(zip(given, held))]
    for load in loads:
        load.start()
    pl.semaphore_wait(barrier, len(neighbours))
    waiting = set(range(INPUTS))

    def need(*numbers):
        for n in numbers:
            if n in waiting:
                waiting.discard(n)
                loads[n].wait()

    def rcopy(src, dst, ss, rs, dev):
        return pltpu.make_async_remote_copy(
            src_ref=src, dst_ref=dst, send_sem=ss, recv_sem=rs, device_id=dev, device_id_type=MESH)

    def got(ref, sem, spare, dev):
        rcopy(ref, ref, spare, sem, dev).wait_recv()

    def sent(ref, sem, spare, dev):
        rcopy(ref, ref, sem, spare, dev).wait_send()

    def rows_2d(ref, start):
        def at(slot, rows):
            return ref.at[pl.ds(pl.multiple_of(slot * k_fs + start, 16), rows), :]
        return at

    def rows_3d(ref, start):
        def at(slot, rows):
            return ref.at[slot, pl.ds(pl.multiple_of(start, 16), rows), :]
        return at

    def whole_2d(ref, rows):
        return ref.at[pl.ds(0, (n_fs - 1) * rows), :]

    def whole_3d(ref, rows):
        return ref.at[pl.ds(0, n_fs - 1), pl.ds(0, rows), :]

    def make(name, ref, three, first, own_rows, swap):
        def at(r, start):
            return (rows_3d if three else rows_2d)(r, first + start)

        whole = whole_3d if three else whole_2d
        result = []
        if pair and swap:
            shared = own_rows - 2 * swap
            result.append(Stream(name + "y", at(ref, par * (own_rows - swap)), swap, whole(ref, swap), True))
            if shared:
                result.append(Stream(name + "b", at(ref, swap), shared, whole(ref, shared), False))
        else:
            result.append(Stream(name + "y", at(ref, 0), own_rows, whole(ref, own_rows), False))
        return result

    streams = {}
    dn_half = k_fs // 2
    for s in (make("uv", wuv, False, 0, k_fs, SWAP["uv"]) + make("out", wout, True, 0, u_w, SWAP["out"])
              + make("up", wup, False, 0, k_fs, SWAP["up"]) + make("e", wdn, False, 0, dn_half, SWAP["e"])
              + make("f", wdn, False, dn_half, dn_half, SWAP["f"])):
        s.index = len(streams)
        streams[s.name] = s

    def z_dirs(s, hop):
        return (0, 1) if hop < half_ring else (s.index % 2,)

    def piece_at(s, d, back):
        return s.ref((f + (n_fs - back if d == 0 else back)) % n_fs, s.rows)

    def z_got(s, d, hop):
        piece = piece_at(s, d, hop)
        got(piece, z_recv.at[s.index, d, hop - 1], z_send.at[s.index], to_up)
        return piece

    def z_send_on(s, d, back, hop, to):
        piece = piece_at(s, d, back)
        rcopy(piece, piece, z_send.at[s.index], z_recv.at[s.index, d, hop - 1], to).start()

    def to_partner(s, piece):
        if s.paired:
            rcopy(piece, piece, y_send.at[s.index], y_recv.at[s.index], to_pair).start()

    def z_hop(name, hop, d):
        s = streams[name]
        if hop > 1 and d in z_dirs(s, hop - 1):
            to_partner(s, z_got(s, d, hop - 1))
        if hop <= half_ring and d in z_dirs(s, hop):
            z_send_on(s, d, hop - 1, hop, to_down if d else to_up)

    def z_even(name, stage, d):
        s = streams[name]
        even = 2 * (stage - 1)
        arrived = stage > 1 and d in z_dirs(s, even)
        if arrived:
            piece = z_got(s, d, even)
        if even < half_ring:
            for step, to in ((2, to_down2 if d else to_up2), (1, to_down if d else to_up)):
                if d in z_dirs(s, even + step):
                    z_send_on(s, d, even, even + step, to)
        if arrived:
            to_partner(s, piece)

    def z_odd(name, stage, d):
        s = streams[name]
        to_partner(s, z_got(s, d, 2 * stage - 3))

    def y_done(name):
        s = streams[name]
        if not s.paired:
            return
        got(s.whole, y_recv.at[s.index], y_send.at[s.index], to_pair)

    def ag_rows(buf, slot, start, rows):
        return buf.at[slot, pl.ds(start, rows), :]

    gathered = (xg, rg, gg)

    def to_other_core(ph, k, piece):
        rcopy(piece, piece, agp_send.at[ph, k], agp_recv.at[ph, k], to_mate).start()

    def ag_a(ph, k):
        need(0)
        buf = gathered[ph]

        def src(at, n):
            return x_ref.at[pl.ds(at, n), :] if ph == 0 else ag_rows(buf, t, at, n)

        for n, to, lo in ((0, to_right, 0), (1, to_right, half), (2, to_left, half), (3, to_left, 0)):
            at = k * chunk + lo
            rcopy(src(at, half), ag_rows(buf, t, at, half), ag_send.at[ph, k], ag_recv.at[ph, k, n], to).start()
        at = k * chunk
        rcopy(src(at, chunk), ag_rows(buf, t, at, chunk), agp_send.at[ph, k], agp_recv.at[ph, k], to_mate).start()

    SIDES = ((n_x - 1, 0, to_right), (1, half, to_left))

    def ag_b(ph, k, side):
        chip_at, lo, to = SIDES[side]
        part = ag_rows(gathered[ph], tp_of(chip_at), k * chunk + lo, half)
        got(part, ag_recv.at[ph, k, 2 * side], ag_send.at[ph, k], to)
        rcopy(part, part, ag_send.at[ph, k], ag_recv.at[ph, k, 4 + side], to).start()

    def ag_c(ph, k, side):
        chip_at, lo, to = SIDES[side]
        part = ag_rows(gathered[ph], tp_of(chip_at), k * chunk + half - lo, half)
        got(part, ag_recv.at[ph, k, 2 * side + 1], ag_send.at[ph, k], to)
        to_other_core(ph, k, ag_rows(gathered[ph], tp_of(chip_at), k * chunk, chunk))

    def ag_e(ph, k, side):
        part = ag_rows(gathered[ph], tp_of(2), k * chunk + SIDES[side][1], half)
        got(part, ag_recv.at[ph, k, 4 + side], ag_send.at[ph, k], to_right)
        to_other_core(ph, k, part)

    def ag_d(ph, k):
        got(gathered[ph].at[pl.ds(0, n_x), pl.ds(k * chunk, chunk), :], agp_recv.at[ph, k], agp_send.at[ph, k], to_mate)

    def a2_s():
        for n, to in enumerate(others):
            rcopy(wout.at[pl.ds(2 * to["tp"], 2)], wmix.at[t], a2_send.at[0], a2_recv.at[0], to).start()
        wmix[t] = wout[pl.ds(2 * t, 2)]

    def a2_w():
        got(wmix.at[pl.ds(0, n_tp - 1)], a2_recv.at[0], a2_send.at[0], to_mate)

    def out_p(k):
        rows = pl.ds(k * chunk, chunk)
        left = jnp.concatenate([gg[j, rows, :] for j in range(n_tp)], axis=1)
        right = jnp.concatenate(
            [jnp.concatenate([wmix[j, 0], wmix[j, 1]], axis=1) for j in range(n_tp)], axis=0)
        total = jnp.dot(left, right, preferred_element_type=F32)
        rg[t, rows, :] = (x_ref[rows, :].astype(F32) + total).astype(BF)

    PAIRS = ((2, 1), (3, 0))

    def product(u, rels, c):
        k, e = u % CHUNKS, u // CHUNKS
        parts = []
        for rel in rels:
            j = chip(rel) * CORES + c
            for shard in (2 * j, 2 * j + 1):
                at = pl.multiple_of(shard * k_fs + e * dn_half, dn_half)
                parts.append(wdn[pl.ds(at, dn_half), :])
        both = lax.dot_general(hid[pl.ds(k * chunk, chunk), :], jnp.concatenate(parts, axis=0),
                               (((1,), (1,)), ((), ())), preferred_element_type=F32)
        return (rels[0], both[:, :k_fs]), (rels[1], both[:, k_fs:])

    def rs_a(k, p):
        for rel, value in product(k, PAIRS[p], 1 - core):
            ps[k, rel] = value.astype(BF)
            rcopy(ps.at[k, rel], pr.at[k, rel], rp_send.at[k], rp_recv.at[k, rel], to_mate).start()

    def rs_b(k, p):
        ss = rr_send.at[k]
        for rel, value in product(k, PAIRS[p], core):
            got(pr.at[k, rel], rp_recv.at[k, rel], rp_send.at[k], to_mate)
            qs[k, rel] = (value + pr[k, rel].astype(F32)).astype(BF)
            low, high = qs.at[k, rel, pl.ds(0, half), :], qs.at[k, rel, pl.ds(half, half), :]
            if rel == 2:
                rcopy(low, op.at[0, k], ss, rr_recv.at[k, 0], to_right).start()
                rcopy(high, op.at[1, k], ss, rr_recv.at[k, 1], to_left).start()
            elif rel == 1:
                rcopy(high, fi.at[0, k, pl.ds(half, half), :], ss, rr_recv.at[k, 2], to_right).start()
            elif rel == 3:
                rcopy(low, fi.at[1, k, pl.ds(0, half), :], ss, rr_recv.at[k, 3], to_left).start()

    def rs_c(k, side):
        ss = rr_send.at[k]
        rel, (_, lo, to) = (1, 3)[side], SIDES[side]
        got(op.at[side, k], rr_recv.at[k, side], ss, to)
        rows = pl.ds(lo, half)
        qs[k, rel, rows, :] = (qs[k, rel, rows, :].astype(F32) + op[side, k].astype(F32)).astype(BF)
        rcopy(qs.at[k, rel, rows, :], fi.at[side, k, rows, :], ss, rr_recv.at[k, 4 + side], to).start()

    def rs_d(k):
        ss = rr_send.at[k]
        for n, side, lo in ((2, 0, half), (3, 1, 0), (4, 0, 0), (5, 1, half)):
            got(fi.at[side, k, pl.ds(lo, half), :], rr_recv.at[k, n], ss, to_right)
        for r in range(0, chunk, ROWS):
            rows, at = pl.ds(r, ROWS), pl.ds((k % CHUNKS) * chunk + r, ROWS)
            total = qs[k, 0, rows, :].astype(F32) + fi[0, k, rows, :].astype(F32) + fi[1, k, rows, :].astype(F32)
            if k < CHUNKS:
                total_e[at, :] = total
            else:
                first, h = total_e[at, :], dn_half
                total = jnp.concatenate([first[:, :h], total[:, :h], first[:, h:], total[:, h:]], axis=1)
                out_ref[at, :] = (rg[t, at, :].astype(F32) + total).astype(BF)

    def column(row):
        return jnp.broadcast_to(row, (row.shape[1], row.shape[1])).T

    def joined(buf, r):
        parts = [buf[j, pl.ds(r, ROWS), :] for j in range(n_tp)]
        squares = None
        for part in parts:
            wide = part.astype(F32)
            squares = wide * wide if squares is None else squares + wide * wide
        inv = lax.rsqrt(jnp.sum(squares, axis=1, keepdims=True) / feats + EPS)
        return jnp.concatenate(parts, axis=1), inv

    def gating(k):
        scale_uv = jnp.concatenate([su_ref[...], sv_ref[...]], axis=1)
        for r in range(0, chunk, ROWS):
            at = k * chunk + r
            lhs, inv = joined(xg, at)
            pre = jnp.dot(lhs, wuv[...], preferred_element_type=F32) * inv * scale_uv
            act = jax.nn.gelu(pre)
            ub[pl.ds(at, ROWS), :] = act[:, :u_w]
            turned = act[:, u_w:].T
            vt[:, pl.ds(at, ROWS)] = turned
            for sums, first in ((jnp.sum(turned, axis=0, keepdims=True), 0),
                                (jnp.sum(turned * turned, axis=0, keepdims=True), chunk // block)):
                for b in range(0, ROWS, block):
                    st[t, k, pl.ds(first + (r + b) // block, 1), :] = sums[:, b:b + block]
        for to in others:
            rcopy(st.at[t, k], st.at[t, k], st_send.at[k], st_recv.at[k], to).start()

    def mixing(k):
        got(st.at[pl.ds(0, n_tp - 1), k], st_recv.at[k], st_send.at[k], to_mate)
        total = st[0, k]
        for n in range(1, n_tp):
            total = total + st[n, k]
        blocks = chunk // block
        mean = total[:blocks] / gm_w
        square = total[blocks:2 * blocks] / gm_w
        scale = lax.rsqrt(square - mean * mean + EPS)
        gain = column(mg_ref[...])[:, 0:1]
        for b in range(0, chunk, block):
            at = k * chunk + b
            n = b // block
            v_norm = ((vt[:, pl.ds(at, block)] - mean[n:n + 1]) * scale[n:n + 1] * gain).astype(BF)
            mixed = lax.dot_general(mask[...], v_norm, (((1,), (1,)), ((), ())), preferred_element_type=F32)
            gg[t, pl.ds(at, block), :] = (ub[pl.ds(at, block), :] * (mixed + bias[...])).astype(BF)

    def ff_up(k):
        for r in range(0, chunk, ROWS):
            at = k * chunk + r
            lhs, inv = joined(rg, at)
            for n in range(0, h_w, 256):
                cols = pl.ds(n, 256)
                acc = jnp.dot(lhs, wup[:, n:n + 256], preferred_element_type=F32)
                acc = jnp.maximum(acc * inv * sup_ref[:, n:n + 256], 0.0)
                hid[pl.ds(at, ROWS), cols] = (acc * acc).astype(BF)

    def rounded(w):
        return w.astype(BF).astype(F32)

    own = pl.ds(pl.multiple_of(f * k_fs, k_fs), k_fs)

    def prep(n):
        if n == 0:
            need(1, 2, 3, 9, 10)
            g1 = column(g1_ref[pl.ds(f, 1), :])
            wuv[own, :] = (jnp.concatenate([rounded(wu_ref[...]) * g1, rounded(wv_ref[...]) * g1], axis=1)).astype(BF)
            wout[f] = (rounded(wo_ref[...]) * so_ref[...]).astype(BF)
        elif n == 1:
            need(11, 12)
            g2 = column(g2_ref[pl.ds(f, 1), :])[:, 0:1]
            wup[own, :] = (rounded(wup_ref[...]) * g2).astype(BF)
        else:
            need(*range(INPUTS))
            wdn[own, :] = (rounded(wdn_ref[...]) * sdn_ref[...]).T.astype(BF)
            xg[t] = x_ref[...]
            at = lax.broadcasted_iota(jnp.int32, (block, block), 0)
            low = at >= lax.broadcasted_iota(jnp.int32, (block, block), 1)
            grp_at = t * u_w // (gm_w // sw_ref.shape[0])
            mask[...] = jnp.where(low, sw_ref[grp_at], 0.0).astype(BF)
            bias[...] = column(sb_ref[pl.ds(grp_at, 1), :])

    steps = {
        "prep": prep, "z": z_hop, "fe": z_even, "fo": z_odd, "yd": y_done, "aga": ag_a, "agb": ag_b, "agc": ag_c,
        "age": ag_e, "agd": ag_d, "gating": gating, "mixing": mixing, "a2s": a2_s, "a2w": a2_w,
        "outp": out_p, "ffup": ff_up, "rsa": rs_a, "rsb": rs_b, "rsc": rs_c, "rsd": rs_d,
    }
    for name, *rest in ORDER:
        steps[name](*rest)

    for s in streams.values():
        sent(s.whole, z_send.at[s.index], z_recv.at[s.index, 0, 0], to_up)
        if s.paired:
            sent(s.whole, y_send.at[s.index], y_recv.at[s.index], to_pair)
    for ph, buf in enumerate(gathered):
        for k in range(CHUNKS):
            rows = pl.ds(k * chunk, chunk)
            sent(buf.at[pl.ds(0, 3), rows, :], ag_send.at[ph, k], ag_recv.at[ph, k, 0], to_right)
            sent(buf.at[pl.ds(0, n_x), rows, :], agp_send.at[ph, k], agp_recv.at[ph, k], to_mate)
    for u in range(2 * CHUNKS):
        sent(ps.at[u], rp_send.at[u], rp_recv.at[u, 0], to_mate)
        sent(qs.at[u, pl.ds(0, 3)], rr_send.at[u], rr_recv.at[u, 0], to_right)
    for k in range(CHUNKS):
        sent(st.at[pl.ds(0, n_tp - 1), k], st_send.at[k], st_recv.at[k], to_mate)
    sent(wmix.at[pl.ds(0, n_tp - 1)], a2_send.at[0], a2_recv.at[0], to_mate)


def per_device(dims, tokens, norm1_gain, weight_u, weight_v, scale_u, scale_v, mix_gain, spatial_weight,
               spatial_bias, weight_out, scale_out, norm2_gain, weight_up, scale_up, weight_down, scale_down):
    n_fs, n_tp = dims["fs"], dims["tp"]
    rows, width = tokens.shape
    feats = width * n_tp
    u_w, h_w = weight_u.shape[1], weight_up.shape[1]
    o_w, d_w = weight_out.shape[1], weight_down.shape[1]
    chunk = rows // CHUNKS
    block = spatial_weight.shape[1]
    n_x = n_tp // CORES
    if n_x != 4 or width != 2 * o_w or width != 2 * d_w:
        raise ValueError("unsupported mesh")
    args = (
        tokens, norm1_gain.reshape(n_fs, -1), weight_u, weight_v,
        scale_u.reshape(1, -1), scale_v.reshape(1, -1), mix_gain.reshape(1, -1), spatial_weight, spatial_bias,
        weight_out, scale_out.reshape(1, -1), norm2_gain.reshape(n_fs, -1), weight_up, scale_up.reshape(1, -1),
        weight_down, scale_down.reshape(1, -1),
    )
    dma = pltpu.SemaphoreType.DMA
    n_streams = 8
    scratch = [
        *[pltpu.VMEM(a.shape, a.dtype) for a in args],
        pltpu.VMEM((feats, 2 * u_w), BF),
        pltpu.VMEM((n_fs, u_w, o_w), BF),
        pltpu.VMEM((feats, h_w), BF),
        pltpu.VMEM((feats, h_w), BF),
        pltpu.VMEM((n_tp, rows, width), BF),
        pltpu.VMEM((n_tp, rows, width), BF),
        pltpu.VMEM((n_tp, rows, u_w), BF),
        pltpu.VMEM((n_tp, 2, u_w, o_w), BF),
        pltpu.VMEM((rows, u_w), F32),
        pltpu.VMEM((u_w, rows), F32),
        pltpu.VMEM((n_tp, CHUNKS, 2 * chunk // block, block), F32),
        pltpu.VMEM((rows, h_w), BF),
        pltpu.VMEM((2 * CHUNKS, n_x, chunk, d_w), BF),
        pltpu.VMEM((2 * CHUNKS, n_x, chunk, d_w), BF),
        pltpu.VMEM((2 * CHUNKS, n_x, chunk, d_w), BF),
        pltpu.VMEM((2, 2 * CHUNKS, chunk // 2, d_w), BF),
        pltpu.VMEM((2, 2 * CHUNKS, chunk, d_w), BF),
        pltpu.VMEM((block, block), BF),
        pltpu.VMEM((block, block), F32),
        pltpu.VMEM((rows, d_w), F32),
        dma((n_streams, 2, n_fs // 2)), dma((n_streams,)), dma((n_streams,)), dma((n_streams,)),
        dma((3, CHUNKS, 6)), dma((3, CHUNKS)), dma((3, CHUNKS)), dma((3, CHUNKS)),
        dma((2 * CHUNKS, n_x)), dma((2 * CHUNKS,)), dma((2 * CHUNKS, 6)), dma((2 * CHUNKS,)),
        dma((CHUNKS,)), dma((CHUNKS,)), dma((1,)), dma((1,)), dma((INPUTS,)),
    ]
    vmem = pl.BlockSpec(memory_space=pltpu.VMEM)
    return pl.pallas_call(
        functools.partial(kernel, dims),
        out_shape=jax.ShapeDtypeStruct(tokens.shape, tokens.dtype),
        in_specs=[pl.BlockSpec(memory_space=pltpu.HBM)] * len(args),
        out_specs=vmem,
        scratch_shapes=scratch,
        name="layer",
        compiler_params=pltpu.CompilerParams(
            collective_id=0, has_side_effects=True, vmem_limit_bytes=64 * 1000 * 1000),
    )(*args)


def solution(mesh):
    placed = (
        P(("grp", "fs"), "tp"), P(), P("fs", "tp"), P("fs", "tp"), P("tp"), P("tp"), P("tp"), P(), P(),
        P("tp", "fs"), P("fs"), P(), P("fs", "tp"), P("tp"), P("tp", "fs"), P("fs"),
    )
    return jax.shard_map(
        functools.partial(per_device, dict(mesh.shape)), mesh=mesh, in_specs=placed,
        out_specs=P(("grp", "fs"), "tp"), check_vma=False)
```

```python
import functools

import jax
import jax.numpy as jnp
from jax import lax
from jax.experimental import pallas as pl
from jax.experimental.pallas import tpu as pltpu
from jax.sharding import PartitionSpec as P

BF = jnp.bfloat16
F32 = jnp.float32
MESH = pl.DeviceIdType.MESH
EPS = 1e-06
CORES = 2
CHUNKS = 2
ROWS = 256
INPUTS = 16
SWAP = {"uv": 64, "out": 64, "up": 48, "e": 16, "f": 16}
ORDER = (
    ("prep", 0), ("fe", "outy", 1, 1), ("fe", "uvy", 1, 0), ("aga", 0, 1), ("fe", "uvy", 1, 1), ("prep", 1),
    ("aga", 0, 0), ("z", "upy", 1, 1), ("z", "upy", 1, 0), ("fe", "outy", 1, 0), ("fo", "outy", 2, 1),
    ("fe", "outy", 2, 1), ("fo", "uvy", 2, 0), ("fe", "uvy", 2, 0), ("prep", 2), ("fe", "uvy", 2, 1),
    ("z", "upy", 2, 0), ("z", "ey", 1, 0), ("z", "upy", 2, 1), ("fo", "uvy", 2, 1), ("z", "ey", 1, 1),
    ("fe", "uvy", 3, 0), ("agb", 0, 0, 1), ("fe", "uvy", 3, 1), ("fe", "outy", 2, 0), ("fo", "uvy", 3, 1),
    ("z", "upb", 1, 1), ("fo", "uvy", 3, 0), ("agb", 0, 1, 0), ("fo", "outy", 2, 0), ("z", "upb", 1, 0),
    ("z", "fb", 1, 1), ("z", "ey", 2, 0), ("agc", 0, 0, 1), ("fe", "uvy", 4, 0), ("agb", 0, 0, 0),
    ("fo", "uvy", 4, 0), ("agb", 0, 1, 1), ("fe", "uvy", 4, 1), ("z", "eb", 1, 0), ("fe", "outy", 3, 1),
    ("fo", "uvy", 4, 1), ("z", "eb", 1, 1), ("agc", 0, 1, 1), ("fe", "outy", 3, 0), ("fo", "uvy", 5, 1),
    ("agc", 0, 1, 0), ("z", "fy", 1, 0), ("z", "upb", 2, 1), ("fo", "uvy", 5, 0), ("age", 0, 0, 1), ("z", "fy", 1, 1),
    ("agc", 0, 0, 0), ("fe", "uvy", 5, 0), ("age", 0, 1, 1), ("age", 0, 0, 0), ("z", "upy", 3, 0),
    ("fe", "outy", 4, 1), ("z", "upy", 3, 1), ("z", "ey", 3, 0), ("age", 0, 1, 0), ("fo", "outy", 3, 1),
    ("fe", "outy", 4, 0), ("agd", 0, 0), ("agd", 0, 1), ("z", "eb", 2, 0), ("fo", "outy", 3, 0), ("z", "upb", 3, 1),
    ("z", "upb", 2, 0), ("yd", "uvy"), ("gating", 0), ("z", "eb", 2, 1), ("fo", "outy", 4, 1), ("gating", 1),
    ("fe", "outy", 5, 1), ("fo", "outy", 4, 0), ("fo", "outy", 5, 0), ("fo", "outy", 5, 1), ("z", "upy", 4, 0),
    ("z", "ey", 2, 1), ("z", "upy", 4, 1), ("z", "eb", 3, 0), ("z", "upb", 4, 1), ("mixing", 0), ("aga", 2, 0),
    ("z", "upb", 3, 0), ("mixing", 1), ("z", "ey", 4, 0), ("z", "upy", 5, 0), ("z", "ey", 3, 1), ("aga", 2, 1),
    ("z", "eb", 3, 1), ("z", "fb", 1, 0), ("yd", "outy"), ("z", "upy", 5, 1), ("agb", 2, 0, 0), ("z", "fy", 2, 0),
    ("agc", 2, 0, 0), ("z", "ey", 4, 1), ("z", "ey", 5, 0), ("z", "eb", 4, 1), ("agb", 2, 0, 1), ("a2s",),
    ("z", "upb", 5, 1), ("agb", 2, 1, 0), ("z", "upy", 6, 0), ("z", "upb", 4, 0), ("agc", 2, 0, 1), ("agb", 2, 1, 1),
    ("z", "upy", 6, 1), ("z", "ey", 6, 0), ("z", "ey", 5, 1), ("z", "fy", 3, 0), ("z", "upy", 7, 0), ("age", 2, 0, 0),
    ("z", "fb", 2, 1), ("age", 2, 0, 1), ("z", "upb", 5, 0), ("z", "eb", 5, 1), ("agc", 2, 1, 1), ("z", "ey", 6, 1),
    ("z", "upy", 7, 1), ("agd", 2, 0), ("z", "ey", 7, 0), ("z", "eb", 4, 0), ("agc", 2, 1, 0), ("age", 2, 1, 1),
    ("z", "upy", 8, 0), ("a2w",), ("outp", 0), ("aga", 1, 0), ("z", "fb", 3, 1), ("age", 2, 1, 0), ("z", "ey", 8, 0),
    ("z", "ey", 7, 1), ("z", "upb", 6, 1), ("z", "eb", 6, 1), ("agd", 2, 1), ("outp", 1), ("z", "fb", 2, 0),
    ("z", "upy", 8, 1), ("z", "eb", 5, 0), ("z", "upy", 9, 0), ("fe", "uvy", 5, 1), ("z", "fy", 2, 1),
    ("z", "ey", 8, 1), ("agb", 1, 0, 1), ("z", "upb", 6, 0), ("agb", 1, 0, 0), ("z", "ey", 9, 0), ("aga", 1, 1),
    ("z", "fy", 4, 0), ("z", "fb", 4, 1), ("z", "upb", 7, 1), ("z", "fb", 3, 0), ("z", "eb", 6, 0), ("z", "fy", 3, 1),
    ("z", "eb", 7, 1), ("z", "fb", 5, 1), ("z", "fy", 5, 0), ("age", 1, 0, 0), ("age", 1, 0, 1), ("z", "upb", 7, 0),
    ("z", "fy", 4, 1), ("z", "fb", 4, 0), ("z", "upb", 8, 1), ("z", "fy", 6, 0), ("agc", 1, 0, 0), ("z", "eb", 8, 1),
    ("agb", 1, 1, 1), ("agc", 1, 0, 1), ("z", "fy", 5, 1), ("z", "fb", 6, 1), ("agb", 1, 1, 0), ("z", "eb", 7, 0),
    ("z", "upb", 8, 0), ("agc", 1, 1, 1), ("agc", 1, 1, 0), ("agd", 1, 0), ("yd", "upy"), ("z", "upb", 9, 1),
    ("z", "fb", 5, 0), ("ffup", 0), ("yd", "ey"), ("z", "eb", 8, 0), ("z", "fy", 6, 1), ("z", "eb", 9, 1),
    ("z", "fy", 7, 0), ("rsa", 0), ("age", 1, 1, 0), ("z", "fb", 6, 0), ("age", 1, 1, 1), ("z", "fb", 7, 1),
    ("rsb", 0, 0), ("rsb", 0, 1), ("z", "fy", 8, 0), ("agd", 1, 1), ("z", "fy", 7, 1), ("ffup", 1), ("z", "fb", 8, 1),
    ("z", "fb", 7, 0), ("rsc", 0, 0), ("z", "fy", 9, 0), ("rsc", 0, 1), ("z", "fy", 8, 1), ("fe", "outy", 5, 0),
    ("rsa", 1), ("rsb", 1, 0), ("rsb", 1, 1), ("z", "fb", 8, 0), ("z", "fb", 9, 1), ("yd", "fy"), ("rsa", 3),
    ("rsd", 0), ("rsb", 3, 0), ("rsc", 1, 0), ("rsc", 1, 1), ("rsa", 2), ("rsb", 3, 1), ("rsb", 2, 0), ("rsc", 3, 0),
    ("rsb", 2, 1), ("rsd", 1), ("rsc", 3, 1), ("rsc", 2, 0), ("rsc", 2, 1), ("rsd", 3), ("rsd", 2),
)


class Stream:
    def __init__(self, name, ref, rows, whole, paired):
        self.name, self.ref, self.rows, self.whole, self.paired = name, ref, rows, whole, paired


def kernel(
    dims,
    *refs,
):
    given, out_ref, held, (
        wuv, wout, wup, wdn, xg, rg, gg, wmix, ub, vt, st, hid,
        ps, pr, qs, op, fi, mine, mask, bias, total_e,
        z_recv, z_send, y_recv, y_send, ag_recv, ag_send, agp_recv, agp_send,
        rp_recv, rp_send, rr_recv, rr_send, st_recv, st_send, a2_recv, a2_send, in_sem,
    ) = refs[:INPUTS], refs[INPUTS], refs[INPUTS + 1:2 * INPUTS + 1], refs[2 * INPUTS + 1:]
    (
        x_ref, g1_ref, wu_ref, wv_ref, su_ref, sv_ref, mg_ref, sw_ref, sb_ref, wo_ref, so_ref,
        g2_ref, wup_ref, sup_ref, wdn_ref, sdn_ref,
    ) = held
    n_fs, n_tp = dims["fs"], dims["tp"]
    n_x = n_tp // CORES
    half_ring = n_fs // 2
    total_rows, width = x_ref.shape
    feats = width * n_tp
    u_w = wu_ref.shape[1]
    k_fs = wu_ref.shape[0]
    h_w = wup_ref.shape[1]
    gm_w = u_w * n_tp
    chunk = total_rows // CHUNKS
    half = chunk // 2
    block = sw_ref.shape[1]
    pair = dims["grp"] % 2 == 0

    g = lax.axis_index("grp")
    f = lax.axis_index("fs")
    t = lax.axis_index("tp")
    cx = t // CORES
    core = t % CORES
    par = g % 2

    def chip(d):
        return (cx + d) % n_x

    def tp_of(d):
        return chip(d) * CORES + core

    to_right, to_left, to_opp = {"tp": tp_of(1)}, {"tp": tp_of(n_x - 1)}, {"tp": tp_of(2)}
    to_mate = {"tp": cx * CORES + 1 - core}
    to_up, to_down = {"fs": (f + 1) % n_fs}, {"fs": (f + n_fs - 1) % n_fs}
    to_pair = {"grp": g + 1 - 2 * par}

    to_up2, to_down2 = {"fs": (f + 2) % n_fs}, {"fs": (f + n_fs - 2) % n_fs}
    others = [{"tp": chip(rel) * CORES + (core + c) % CORES} for rel in range(n_x) for c in range(CORES) if rel or c]
    neighbours = others + [to_up, to_down, to_up2, to_down2]
    if pair:
        neighbours.append(to_pair)
    barrier = pltpu.get_barrier_semaphore()
    for n in neighbours:
        pl.semaphore_signal(barrier, inc=1, device_id=n, device_id_type=MESH)
    loads = [pltpu.make_async_copy(a, b, in_sem.at[n]) for n, (a, b) in enumerate(zip(given, held))]
    for load in loads:
        load.start()
    pl.semaphore_wait(barrier, len(neighbours))
    waiting = set(range(INPUTS))

    def need(*numbers):
        for n in numbers:
            if n in waiting:
                waiting.discard(n)
                loads[n].wait()

    def rcopy(src, dst, ss, rs, dev):
        return pltpu.make_async_remote_copy(
            src_ref=src, dst_ref=dst, send_sem=ss, recv_sem=rs, device_id=dev, device_id_type=MESH)

    def got(ref, sem, spare, dev):
        rcopy(ref, ref, spare, sem, dev).wait_recv()

    def sent(ref, sem, spare, dev):
        rcopy(ref, ref, sem, spare, dev).wait_send()

    def rows_2d(ref, start):
        def at(slot, rows):
            return ref.at[pl.ds(pl.multiple_of(slot * k_fs + start, 16), rows), :]
        return at

    def rows_3d(ref, start):
        def at(slot, rows):
            return ref.at[slot, pl.ds(pl.multiple_of(start, 16), rows), :]
        return at

    def whole_2d(ref, rows):
        return ref.at[pl.ds(0, (n_fs - 1) * rows), :]

    def whole_3d(ref, rows):
        return ref.at[pl.ds(0, n_fs - 1), pl.ds(0, rows), :]

    def make(name, ref, three, first, own_rows, swap):
        def at(r, start):
            return (rows_3d if three else rows_2d)(r, first + start)

        whole = whole_3d if three else whole_2d
        result = []
        if pair and swap:
            shared = own_rows - 2 * swap
            result.append(Stream(name + "y", at(ref, par * (own_rows - swap)), swap, whole(ref, swap), True))
            if shared:
                result.append(Stream(name + "b", at(ref, swap), shared, whole(ref, shared), False))
        else:
            result.append(Stream(name + "y", at(ref, 0), own_rows, whole(ref, own_rows), False))
        return result

    streams = {}
    dn_half = k_fs // 2
    for s in (make("uv", wuv, False, 0, k_fs, SWAP["uv"]) + make("out", wout, True, 0, u_w, SWAP["out"])
              + make("up", wup, False, 0, k_fs, SWAP["up"]) + make("e", wdn, False, 0, dn_half, SWAP["e"])
              + make("f", wdn, False, dn_half, dn_half, SWAP["f"])):
        s.index = len(streams)
        streams[s.name] = s

    def z_dirs(s, hop):
        return (0, 1) if hop < half_ring else (s.index % 2,)

    def piece_at(s, d, back):
        return s.ref((f + (n_fs - back if d == 0 else back)) % n_fs, s.rows)

    def z_got(s, d, hop):
        piece = piece_at(s, d, hop)
        got(piece, z_recv.at[s.index, d, hop - 1], z_send.at[s.index], to_up)
        return piece

    def z_send_on(s, d, back, hop, to):
        piece = piece_at(s, d, back)
        rcopy(piece, piece, z_send.at[s.index], z_recv.at[s.index, d, hop - 1], to).start()

    def to_partner(s, piece):
        if s.paired:
            rcopy(piece, piece, y_send.at[s.index], y_recv.at[s.index], to_pair).start()

    def z_hop(name, hop, d):
        s = streams[name]
        if hop > 1 and d in z_dirs(s, hop - 1):
            to_partner(s, z_got(s, d, hop - 1))
        if hop <= half_ring and d in z_dirs(s, hop):
            z_send_on(s, d, hop - 1, hop, to_down if d else to_up)

    def z_even(name, stage, d):
        s = streams[name]
        even = 2 * (stage - 1)
        arrived = stage > 1 and d in z_dirs(s, even)
        if arrived:
            piece = z_got(s, d, even)
        if even < half_ring:
            for step, to in ((2, to_down2 if d else to_up2), (1, to_down if d else to_up)):
                if d in z_dirs(s, even + step):
                    z_send_on(s, d, even, even + step, to)
        if arrived:
            to_partner(s, piece)

    def z_odd(name, stage, d):
        s = streams[name]
        to_partner(s, z_got(s, d, 2 * stage - 3))

    def y_done(name):
        s = streams[name]
        if not s.paired:
            return
        got(s.whole, y_recv.at[s.index], y_send.at[s.index], to_pair)

    def ag_rows(buf, slot, start, rows):
        return buf.at[slot, pl.ds(start, rows), :]

    gathered = (xg, rg, gg)

    def to_other_core(ph, k, piece):
        rcopy(piece, piece, agp_send.at[ph, k], agp_recv.at[ph, k], to_mate).start()

    def ag_a(ph, k):
        need(0)
        buf = gathered[ph]

        def src(at, n):
            return x_ref.at[pl.ds(at, n), :] if ph == 0 else ag_rows(buf, t, at, n)

        for n, to, lo in ((0, to_right, 0), (1, to_right, half), (2, to_left, half), (3, to_left, 0)):
            at = k * chunk + lo
            rcopy(src(at, half), ag_rows(buf, t, at, half), ag_send.at[ph, k], ag_recv.at[ph, k, n], to).start()
        at = k * chunk
        rcopy(src(at, chunk), ag_rows(buf, t, at, chunk), agp_send.at[ph, k], agp_recv.at[ph, k], to_mate).start()

    SIDES = ((n_x - 1, 0, to_right), (1, half, to_left))

    def ag_b(ph, k, side):
        chip_at, lo, to = SIDES[side]
        part = ag_rows(gathered[ph], tp_of(chip_at), k * chunk + lo, half)
        got(part, ag_recv.at[ph, k, 2 * side], ag_send.at[ph, k], to)
        rcopy(part, part, ag_send.at[ph, k], ag_recv.at[ph, k, 4 + side], to).start()

    def ag_c(ph, k, side):
        chip_at, lo, to = SIDES[side]
        part = ag_rows(gathered[ph], tp_of(chip_at), k * chunk + half - lo, half)
        got(part, ag_recv.at[ph, k, 2 * side + 1], ag_send.at[ph, k], to)
        to_other_core(ph, k, ag_rows(gathered[ph], tp_of(chip_at), k * chunk, chunk))

    def ag_e(ph, k, side):
        part = ag_rows(gathered[ph], tp_of(2), k * chunk + SIDES[side][1], half)
        got(part, ag_recv.at[ph, k, 4 + side], ag_send.at[ph, k], to_right)
        to_other_core(ph, k, part)

    def ag_d(ph, k):
        got(gathered[ph].at[pl.ds(0, n_x), pl.ds(k * chunk, chunk), :], agp_recv.at[ph, k], agp_send.at[ph, k], to_mate)

    def a2_s():
        for n, to in enumerate(others):
            rcopy(wout.at[pl.ds(2 * to["tp"], 2)], wmix.at[t], a2_send.at[0], a2_recv.at[0], to).start()
        wmix[t] = wout[pl.ds(2 * t, 2)]

    def a2_w():
        got(wmix.at[pl.ds(0, n_tp - 1)], a2_recv.at[0], a2_send.at[0], to_mate)

    def out_p(k):
        rows = pl.ds(k * chunk, chunk)
        left = jnp.concatenate([gg[j, rows, :] for j in range(n_tp)], axis=1)
        right = jnp.concatenate(
            [jnp.concatenate([wmix[j, 0], wmix[j, 1]], axis=1) for j in range(n_tp)], axis=0)
        total = jnp.dot(left, right, preferred_element_type=F32)
        rg[t, rows, :] = (x_ref[rows, :].astype(F32) + total).astype(BF)

    PAIRS = ((2, 1), (3, 0))

    def product(u, rels, c):
        k, e = u % CHUNKS, u // CHUNKS
        parts = []
        for rel in rels:
            j = chip(rel) * CORES + c
            for shard in (2 * j, 2 * j + 1):
                at = pl.multiple_of(shard * k_fs + e * dn_half, dn_half)
                parts.append(wdn[pl.ds(at, dn_half), :])
        return lax.dot_general(hid[pl.ds(k * chunk, chunk), :], jnp.concatenate(parts, axis=0),
                               (((1,), (1,)), ((), ())), preferred_element_type=F32)

    def rs_a(k):
        for rels in PAIRS:
            both = product(k, rels, 1 - core)
            for n, rel in enumerate(rels):
                ps[k, rel] = both[:, n * k_fs:(n + 1) * k_fs].astype(BF)
                rcopy(ps.at[k, rel], pr.at[k, rel], rp_send.at[k], rp_recv.at[k, rel], to_mate).start()
        for p, rels in enumerate(PAIRS):
            mine[k, p] = product(k, rels, core)

    def rs_b(k, p):
        ss = rr_send.at[k]
        for n, rel in enumerate(PAIRS[p]):
            got(pr.at[k, rel], rp_recv.at[k, rel], rp_send.at[k], to_mate)
            qs[k, rel] = (mine[k, p, :, n * k_fs:(n + 1) * k_fs] + pr[k, rel].astype(F32)).astype(BF)
            low, high = qs.at[k, rel, pl.ds(0, half), :], qs.at[k, rel, pl.ds(half, half), :]
            if rel == 2:
                rcopy(low, op.at[0, k], ss, rr_recv.at[k, 0], to_right).start()
                rcopy(high, op.at[1, k], ss, rr_recv.at[k, 1], to_left).start()
            elif rel == 1:
                rcopy(high, fi.at[0, k, pl.ds(half, half), :], ss, rr_recv.at[k, 2], to_right).start()
            elif rel == 3:
                rcopy(low, fi.at[1, k, pl.ds(0, half), :], ss, rr_recv.at[k, 3], to_left).start()

    def rs_c(k, side):
        ss = rr_send.at[k]
        rel, (_, lo, to) = (1, 3)[side], SIDES[side]
        got(op.at[side, k], rr_recv.at[k, side], ss, to)
        rows = pl.ds(lo, half)
        qs[k, rel, rows, :] = (qs[k, rel, rows, :].astype(F32) + op[side, k].astype(F32)).astype(BF)
        rcopy(qs.at[k, rel, rows, :], fi.at[side, k, rows, :], ss, rr_recv.at[k, 4 + side], to).start()

    def rs_d(k):
        ss = rr_send.at[k]
        for n, side, lo in ((2, 0, half), (3, 1, 0), (4, 0, 0), (5, 1, half)):
            got(fi.at[side, k, pl.ds(lo, half), :], rr_recv.at[k, n], ss, to_right)
        for r in range(0, chunk, ROWS):
            rows, at = pl.ds(r, ROWS), pl.ds((k % CHUNKS) * chunk + r, ROWS)
            total = qs[k, 0, rows, :].astype(F32) + fi[0, k, rows, :].astype(F32) + fi[1, k, rows, :].astype(F32)
            if k < CHUNKS:
                total_e[at, :] = total
            else:
                first, h = total_e[at, :], dn_half
                total = jnp.concatenate([first[:, :h], total[:, :h], first[:, h:], total[:, h:]], axis=1)
                out_ref[at, :] = (rg[t, at, :].astype(F32) + total).astype(BF)

    def column(row):
        return jnp.broadcast_to(row, (row.shape[1], row.shape[1])).T

    def joined(buf, r):
        parts = [buf[j, pl.ds(r, ROWS), :] for j in range(n_tp)]
        squares = None
        for part in parts:
            wide = part.astype(F32)
            squares = wide * wide if squares is None else squares + wide * wide
        inv = lax.rsqrt(jnp.sum(squares, axis=1, keepdims=True) / feats + EPS)
        return jnp.concatenate(parts, axis=1), inv

    def gating(k):
        scale_uv = jnp.concatenate([su_ref[...], sv_ref[...]], axis=1)
        for r in range(0, chunk, ROWS):
            at = k * chunk + r
            lhs, inv = joined(xg, at)
            pre = jnp.dot(lhs, wuv[...], preferred_element_type=F32) * inv * scale_uv
            act = jax.nn.gelu(pre)
            ub[pl.ds(at, ROWS), :] = act[:, :u_w]
            turned = act[:, u_w:].T
            vt[:, pl.ds(at, ROWS)] = turned
            for sums, first in ((jnp.sum(turned, axis=0, keepdims=True), 0),
                                (jnp.sum(turned * turned, axis=0, keepdims=True), chunk // block)):
                for b in range(0, ROWS, block):
                    st[t, k, pl.ds(first + (r + b) // block, 1), :] = sums[:, b:b + block]
        for to in others:
            rcopy(st.at[t, k], st.at[t, k], st_send.at[k], st_recv.at[k], to).start()

    def mixing(k):
        got(st.at[pl.ds(0, n_tp - 1), k], st_recv.at[k], st_send.at[k], to_mate)
        total = st[0, k]
        for n in range(1, n_tp):
            total = total + st[n, k]
        blocks = chunk // block
        mean = total[:blocks] / gm_w
        square = total[blocks:2 * blocks] / gm_w
        scale = lax.rsqrt(square - mean * mean + EPS)
        gain = column(mg_ref[...])[:, 0:1]
        for b in range(0, chunk, block):
            at = k * chunk + b
            n = b // block
            v_norm = ((vt[:, pl.ds(at, block)] - mean[n:n + 1]) * scale[n:n + 1] * gain).astype(BF)
            mixed = lax.dot_general(mask[...], v_norm, (((1,), (1,)), ((), ())), preferred_element_type=F32)
            gg[t, pl.ds(at, block), :] = (ub[pl.ds(at, block), :] * (mixed + bias[...])).astype(BF)

    def ff_up(k):
        for r in range(0, chunk, ROWS):
            at = k * chunk + r
            lhs, inv = joined(rg, at)
            for n in range(0, h_w, 256):
                cols = pl.ds(n, 256)
                acc = jnp.dot(lhs, wup[:, n:n + 256], preferred_element_type=F32)
                acc = jnp.maximum(acc * inv * sup_ref[:, n:n + 256], 0.0)
                hid[pl.ds(at, ROWS), cols] = (acc * acc).astype(BF)

    def rounded(w):
        return w.astype(BF).astype(F32)

    own = pl.ds(pl.multiple_of(f * k_fs, k_fs), k_fs)

    def prep(n):
        if n == 0:
            need(1, 2, 3, 9, 10)
            g1 = column(g1_ref[pl.ds(f, 1), :])
            wuv[own, :] = (jnp.concatenate([rounded(wu_ref[...]) * g1, rounded(wv_ref[...]) * g1], axis=1)).astype(BF)
            wout[f] = (rounded(wo_ref[...]) * so_ref[...]).astype(BF)
        elif n == 1:
            need(11, 12)
            g2 = column(g2_ref[pl.ds(f, 1), :])[:, 0:1]
            wup[own, :] = (rounded(wup_ref[...]) * g2).astype(BF)
        else:
            need(*range(INPUTS))
            wdn[own, :] = (rounded(wdn_ref[...]) * sdn_ref[...]).T.astype(BF)
            xg[t] = x_ref[...]
            at = lax.broadcasted_iota(jnp.int32, (block, block), 0)
            low = at >= lax.broadcasted_iota(jnp.int32, (block, block), 1)
            grp_at = t * u_w // (gm_w // sw_ref.shape[0])
            mask[...] = jnp.where(low, sw_ref[grp_at], 0.0).astype(BF)
            bias[...] = column(sb_ref[pl.ds(grp_at, 1), :])

    steps = {
        "prep": prep, "z": z_hop, "fe": z_even, "fo": z_odd, "yd": y_done, "aga": ag_a, "agb": ag_b, "agc": ag_c,
        "age": ag_e, "agd": ag_d, "gating": gating, "mixing": mixing, "a2s": a2_s, "a2w": a2_w,
        "outp": out_p, "ffup": ff_up, "rsa": rs_a, "rsb": rs_b, "rsc": rs_c, "rsd": rs_d,
    }
    for name, *rest in ORDER:
        steps[name](*rest)

    for s in streams.values():
        sent(s.whole, z_send.at[s.index], z_recv.at[s.index, 0, 0], to_up)
        if s.paired:
            sent(s.whole, y_send.at[s.index], y_recv.at[s.index], to_pair)
    for ph, buf in enumerate(gathered):
        for k in range(CHUNKS):
            rows = pl.ds(k * chunk, chunk)
            sent(buf.at[pl.ds(0, 3), rows, :], ag_send.at[ph, k], ag_recv.at[ph, k, 0], to_right)
            sent(buf.at[pl.ds(0, n_x), rows, :], agp_send.at[ph, k], agp_recv.at[ph, k], to_mate)
    for u in range(2 * CHUNKS):
        sent(ps.at[u], rp_send.at[u], rp_recv.at[u, 0], to_mate)
        sent(qs.at[u, pl.ds(0, 3)], rr_send.at[u], rr_recv.at[u, 0], to_right)
    for k in range(CHUNKS):
        sent(st.at[pl.ds(0, n_tp - 1), k], st_send.at[k], st_recv.at[k], to_mate)
    sent(wmix.at[pl.ds(0, n_tp - 1)], a2_send.at[0], a2_recv.at[0], to_mate)


def per_device(dims, tokens, norm1_gain, weight_u, weight_v, scale_u, scale_v, mix_gain, spatial_weight,
               spatial_bias, weight_out, scale_out, norm2_gain, weight_up, scale_up, weight_down, scale_down):
    n_fs, n_tp = dims["fs"], dims["tp"]
    rows, width = tokens.shape
    feats = width * n_tp
    u_w, h_w = weight_u.shape[1], weight_up.shape[1]
    o_w, d_w = weight_out.shape[1], weight_down.shape[1]
    chunk = rows // CHUNKS
    block = spatial_weight.shape[1]
    n_x = n_tp // CORES
    if n_x != 4 or width != 2 * o_w or width != 2 * d_w:
        raise ValueError("unsupported mesh")
    args = (
        tokens, norm1_gain.reshape(n_fs, -1), weight_u, weight_v,
        scale_u.reshape(1, -1), scale_v.reshape(1, -1), mix_gain.reshape(1, -1), spatial_weight, spatial_bias,
        weight_out, scale_out.reshape(1, -1), norm2_gain.reshape(n_fs, -1), weight_up, scale_up.reshape(1, -1),
        weight_down, scale_down.reshape(1, -1),
    )
    dma = pltpu.SemaphoreType.DMA
    n_streams = 8
    scratch = [
        *[pltpu.VMEM(a.shape, a.dtype) for a in args],
        pltpu.VMEM((feats, 2 * u_w), BF),
        pltpu.VMEM((n_fs, u_w, o_w), BF),
        pltpu.VMEM((feats, h_w), BF),
        pltpu.VMEM((feats, h_w), BF),
        pltpu.VMEM((n_tp, rows, width), BF),
        pltpu.VMEM((n_tp, rows, width), BF),
        pltpu.VMEM((n_tp, rows, u_w), BF),
        pltpu.VMEM((n_tp, 2, u_w, o_w), BF),
        pltpu.VMEM((rows, u_w), F32),
        pltpu.VMEM((u_w, rows), F32),
        pltpu.VMEM((n_tp, CHUNKS, 2 * chunk // block, block), F32),
        pltpu.VMEM((rows, h_w), BF),
        pltpu.VMEM((2 * CHUNKS, n_x, chunk, d_w), BF),
        pltpu.VMEM((2 * CHUNKS, n_x, chunk, d_w), BF),
        pltpu.VMEM((2 * CHUNKS, n_x, chunk, d_w), BF),
        pltpu.VMEM((2, 2 * CHUNKS, chunk // 2, d_w), BF),
        pltpu.VMEM((2, 2 * CHUNKS, chunk, d_w), BF),
        pltpu.VMEM((2 * CHUNKS, 2, chunk, 2 * d_w), F32),
        pltpu.VMEM((block, block), BF),
        pltpu.VMEM((block, block), F32),
        pltpu.VMEM((rows, d_w), F32),
        dma((n_streams, 2, n_fs // 2)), dma((n_streams,)), dma((n_streams,)), dma((n_streams,)),
        dma((3, CHUNKS, 6)), dma((3, CHUNKS)), dma((3, CHUNKS)), dma((3, CHUNKS)),
        dma((2 * CHUNKS, n_x)), dma((2 * CHUNKS,)), dma((2 * CHUNKS, 6)), dma((2 * CHUNKS,)),
        dma((CHUNKS,)), dma((CHUNKS,)), dma((1,)), dma((1,)), dma((INPUTS,)),
    ]
    vmem = pl.BlockSpec(memory_space=pltpu.VMEM)
    return pl.pallas_call(
        functools.partial(kernel, dims),
        out_shape=jax.ShapeDtypeStruct(tokens.shape, tokens.dtype),
        in_specs=[pl.BlockSpec(memory_space=pltpu.HBM)] * len(args),
        out_specs=vmem,
        scratch_shapes=scratch,
        name="layer",
        compiler_params=pltpu.CompilerParams(
            collective_id=0, has_side_effects=True, vmem_limit_bytes=64 * 1000 * 1000),
    )(*args)


def solution(mesh):
    placed = (
        P(("grp", "fs"), "tp"), P(), P("fs", "tp"), P("fs", "tp"), P("tp"), P("tp"), P("tp"), P(), P(),
        P("tp", "fs"), P("fs"), P(), P("fs", "tp"), P("tp"), P("tp", "fs"), P("fs"),
    )
    return jax.shard_map(
        functools.partial(per_device, dict(mesh.shape)), mesh=mesh, in_specs=placed,
        out_specs=P(("grp", "fs"), "tp"), check_vma=False)
```
